512 devices in a mesh: ep: 32 (over z, x), tp: 16 (over y, core).
Axes of the slice: x: 4, y: 8, z: 8, core: 2. Of those that a mesh axis runs over, the one named last changes fastest.
Arguments:
- mixer_tokens: bfloat16 [6144, 2048], P('ep'), may hold values from -6 to 6
- mixer_gain: float32 [2048], replicated, may hold values from 0.1 to 1.9
- query_weight: bfloat16 [1024, 2048], P('tp'), may hold values from -1 to 1
- key_weight: bfloat16 [1024, 2048], P('tp'), may hold values from -1 to 1
- value_weight: bfloat16 [1024, 2048], P('tp'), may hold values from -0.125 to 0.125
- forget_weight: bfloat16 [2048, 16], P(None, 'tp'), may hold values from -0.125 to 0.125
- forget_bias: float32 [32, 16], P('ep', 'tp'), may hold values from 2.98 to 10.4
- output_weight: bfloat16 [1024, 2048], P(None, 'tp'), may hold values from -0.1875 to 0.1875
- expert_tokens: bfloat16 [4096, 2048], P('ep'), may hold values from -6 to 6
- expert_gain: float32 [2048], replicated, may hold values from 0.1 to 1.9
- routes: int32 [4096, 2], P('ep'), may hold values from 0 to 31, all different within a row; in each aligned block of 128 rows (0 to 127, 128 to 255, ...) at most 16 rows name the same one
- route_weights: float32 [4096, 2], P('ep'), may hold values from 0.2 to 1
- gate_weight: bfloat16 [32, 3584, 2048], P('ep', 'tp'), may hold values from -0.125 to 0.125
- up_weight: bfloat16 [32, 3584, 2048], P('ep', 'tp'), may hold values from -0.125 to 0.125
- down_weight: bfloat16 [32, 3584, 2048], P('ep', 'tp'), may hold values from -0.09375 to 0.09375
Outputs:
- mixer_output: bfloat16 [6144, 2048], P('ep', 'tp')
- expert_output: bfloat16 [4096, 2048], P('ep', 'tp')
The draws below stay inside these ranges and needn't reach their ends.
Inputs may be any that keep to these rules, and one draw needn't show every extreme that they name: `routes`: within the tokens of one index of ep (aligned blocks of 128 rows) no expert is named more than 16 times, a bound that some block reaches; the 2 experts of a token differ.
All inputs are finite; a program needn't handle non-finite values.
Results may differ from the reference program's by a relative error of at most 0.019.
Values may be sent and summed in bfloat16 or wider, within the bound.
A program may use at most 128 MiB of HBM per device.

```python
import math
import jax
import jax.numpy as jnp
import numpy as np
from jax import lax

D = 2048
HEADS = 16
HD = 64
EXPERT_FF = 3584
TOP = 2
TOK_A = 192
TOK_B = 128
EXPERTS = 32
CAP = 16
TOKENS_A = 6144
TOKENS_B = 4096
N_EP = 32
N_TP = 16


def spiked_weight(key, salt):
    base_draw = jax.random.normal(jax.random.fold_in(key, salt), (HEADS * HD, D), jnp.float32)
    base_draw = jnp.clip(base_draw, -6.0, 6.0) * D ** (-0.5)
    return base_draw.astype(jnp.bfloat16)


def draw_query_weight(key, part):
    return spiked_weight(key, 11)


def draw_key_weight(key, part):
    return spiked_weight(key, 12)


def draw_mixer_tokens(key, part):
    values = jnp.clip(jax.random.normal(jax.random.fold_in(key, 201), (TOKENS_A, D), jnp.float32), -6.0, 6.0)
    return values.astype(jnp.bfloat16)


def draw_forget_bias(key, part):
    block_count = TOKENS_A // TOK_A
    chance = 0.5
    slow_heads = jax.random.bernoulli(jax.random.fold_in(key, 301), chance, (HEADS,))
    base_level = jnp.where(slow_heads, 9.7, math.log(40.0)).astype(jnp.float32)
    block_drift = jax.random.uniform(jax.random.fold_in(key, 302), (block_count, HEADS), jnp.float32, -0.7, 0.7)
    return base_level[None, :] + block_drift


def steps_of(rng, shape, split, least, largest):
    factor_of = 1.0
    for axis_at, blocks in split:
        draws = jax.random.uniform(jax.random.fold_in(jax.random.fold_in(rng, 6), axis_at), (blocks,), jnp.float32, least / len(split), largest / len(split))
        factor_of = factor_of * jnp.repeat(jnp.exp(draws), shape[axis_at] // blocks).reshape((-1,) + (1,) * (len(shape) - 1 - axis_at))
    return factor_of


def deal_out(rng, own, number, rows, count, top, limit, lean):
    order = jax.random.permutation(rng, count)
    heavy_load, common = portions_of(count, rows * top, limit, lean, True), portions_of(count, rows * top, limit, lean, False)
    places = jnp.arange(count)

    def named(tallies, offset_by):
        used = int((tallies > 0).sum())
        fixed = max(1, used // 4)
        moved = fixed + (places - fixed + offset_by * (used - fixed)) % max(1, count - fixed)
        return jnp.zeros((count,), jnp.int32).at[order[jnp.where(places < fixed, places, moved)]].set(jnp.asarray(tallies, jnp.int32))

    tallies = jnp.where(number % 4 == 0, named(heavy_load, number // 4), named(common, number - number // 4 - 1))
    mixed = jax.random.permutation(jax.random.fold_in(own, 3), count)
    source_of, sink = mixed[0:count // 2 * 2:2], mixed[1:count // 2 * 2:2]
    margin = jnp.minimum(tallies[source_of] - 1, limit - tallies[sink]) // 2
    margin = jnp.where((source_of == order[0]) | (sink == order[0]) | (tallies[sink] == 0), 0, jnp.maximum(margin, 0))
    moved = jax.random.randint(jax.random.fold_in(own, 4), (count // 2,), 0, 1 << 20) % (margin + 1)
    tallies = tallies.at[source_of].add(-moved).at[sink].add(moved)
    members = jnp.searchsorted(jnp.cumsum(tallies), jnp.arange(rows * top), side="right").astype(jnp.int32)
    listing = members.reshape(top, rows).T
    listing = listing[jax.random.permutation(jax.random.fold_in(own, 1), rows)]
    offset_by = jax.random.randint(jax.random.fold_in(own, 2), (rows, 1), 0, top)
    return jnp.take_along_axis(listing, (jnp.arange(top)[None, :] + offset_by) % top, axis=1)


def portions_of(count, total, most, lean, full):
    loads = [(1 << 20) // math.isqrt(grade ** lean) + 1 for grade in range(1, count + 1)]
    largest = most if full else min(most, max(-(-total // count), total * loads[0] // sum(loads)))
    least = 1 if total - largest >= count - 1 else 0
    given, rest = [largest] + [least] * (count - 1), total - largest - least * (count - 1)
    while rest > 0:
        free = [i for i in range(1, count) if given[i] < largest] or [i for i in range(1, count) if given[i] < most]
        mass, remaining = sum([loads[i] for i in free]), rest
        for i in free:
            extra = min(most - given[i], max(1, remaining * loads[i] // mass), rest)
            given[i] = given[i] + extra
            rest = rest - extra
    return np.array(given)


def centred(rng, dims, width, most, cuts=(), kind=jnp.bfloat16):
    values = jax.random.normal(rng, dims, jnp.float32) * width
    if len(cuts) > 0:
        values = steps_of(rng, dims, cuts, -0.22, 0.18) * values
    return jnp.clip(values, min=-most, max=most).astype(kind)


def setup_inputs(seed: int = 0) -> dict:
    splits = jax.random.split(jax.random.key(seed), 16)
    mixer_tokens = draw_mixer_tokens(jax.random.fold_in(splits[15], 71), 0)
    mixer_gain = jnp.clip(1.0 + 0.18 * jax.random.normal(splits[1], (D,), jnp.float32), 0.1, 1.9)
    query_weight = draw_query_weight(jax.random.fold_in(splits[15], 71), 0)
    key_weight = draw_key_weight(jax.random.fold_in(splits[15], 71), 0)
    value_weight = centred(splits[4], (HEADS * HD, D), D ** -0.5, 0.125, ((0, 16),))
    forget_weight = centred(splits[5], (D, HEADS), D ** -0.5, 0.125, ((1, 16),))
    forget_bias = draw_forget_bias(jax.random.fold_in(splits[15], 71), 0)
    output_weight = centred(splits[7], (HEADS * HD, D), (HEADS * HD) ** -0.5, 0.1875, ((1, 16),))
    expert_tokens = centred(splits[8], (TOKENS_B, D), 1.0, 6.0, ((0, 32),))
    expert_gain = jnp.clip(1.0 + 0.18 * jax.random.normal(splits[9], (D,), jnp.float32), 0.1, 1.9)
    routes_keys = jax.random.split(jax.random.fold_in(splits[10], 1), TOKENS_B // TOK_B)
    routes_turns = jax.random.permutation(jax.random.fold_in(splits[10], 3), TOKENS_B // TOK_B)
    routes = jax.vmap(lambda own, number: deal_out(jax.random.fold_in(splits[10], 2), own, number, TOK_B, EXPERTS, TOP, CAP, 2))(routes_keys, routes_turns).reshape((TOKENS_B, TOP))
    route_weights = jnp.clip(0.2 + 0.8 * jax.random.uniform(splits[11], (TOKENS_B, TOP), jnp.float32) ** steps_of(splits[11], (TOKENS_B, TOP), ((0, 32),), -0.2, 0.2), 0.2, 1.0)
    gate_weight = centred(splits[12], (EXPERTS, EXPERT_FF, D), D ** -0.5, 0.125, ((0, 32), (1, 16)))
    up_weight = centred(splits[13], (EXPERTS, EXPERT_FF, D), D ** -0.5, 0.125, ((0, 32), (1, 16)))
    down_weight = centred(splits[14], (EXPERTS, EXPERT_FF, D), EXPERT_FF ** -0.5, 0.09375, ((0, 32), (1, 16)))
    return {"mixer_tokens": mixer_tokens, "mixer_gain": mixer_gain, "query_weight": query_weight, "key_weight": key_weight, "value_weight": value_weight, "forget_weight": forget_weight, "forget_bias": forget_bias, "output_weight": output_weight, "expert_tokens": expert_tokens, "expert_gain": expert_gain, "routes": routes, "route_weights": route_weights, "gate_weight": gate_weight, "up_weight": up_weight, "down_weight": down_weight}


MEAN_FLOOR = 0.1
HEAD_FLOOR = 1.0

def normed_rows(inputs, gain):
    values = inputs.astype(jnp.float32)
    square = lax.optimization_barrier(jnp.mean(values * values, axis=-1, keepdims=True))
    return (values * lax.rsqrt(jnp.maximum(square, MEAN_FLOOR)) * gain).astype(jnp.bfloat16)

def by_rows(left, weight):
    return lax.dot_general(left, weight, (((1,), (1,)), ((), ())), preferred_element_type=jnp.float32)

def reference(mixer_tokens, mixer_gain, query_weight, key_weight, value_weight, forget_weight, forget_bias, output_weight, expert_tokens, expert_gain, routes, route_weights, gate_weight, up_weight, down_weight):
    sequence = mixer_tokens.shape[0]
    normed = normed_rows(mixer_tokens, mixer_gain)
    queries = by_rows(normed, query_weight).astype(jnp.bfloat16)
    key_rows = by_rows(normed, key_weight).astype(jnp.bfloat16)
    value_rows = by_rows(normed, value_weight).astype(jnp.bfloat16)
    pre_gate = jnp.dot(normed, forget_weight, preferred_element_type=jnp.float32)
    pre_gate = pre_gate + jnp.repeat(forget_bias, TOK_A, axis=0)
    cumulative = jnp.cumsum(jax.nn.log_sigmoid(pre_gate), axis=0)
    head_query = queries.reshape(sequence, HEADS, HD).astype(jnp.float32)
    head_keys = key_rows.reshape(sequence, HEADS, HD).astype(jnp.float32)
    head_values = value_rows.reshape(sequence, HEADS, HD).astype(jnp.float32)
    key_pos = jnp.arange(sequence, dtype=jnp.int32)

    def attend_block(number):
        first_row = (number * TOK_A).astype(jnp.int32)
        block_query = lax.dynamic_slice_in_dim(head_query, first_row, TOK_A, 0)
        block_cum = lax.dynamic_slice_in_dim(cumulative, first_row, TOK_A, 0)
        scores = jnp.einsum('qhd,khd->hqk', block_query, head_keys) * HD ** (-0.5)
        scores = scores + block_cum.T[:, :, None] - cumulative.T[:, None, :]
        query_pos = first_row + jnp.arange(TOK_A, dtype=jnp.int32)
        scores = jnp.where(key_pos[None, None, :] <= query_pos[None, :, None], scores, -jnp.inf)
        row_max = lax.optimization_barrier(jnp.max(scores, axis=-1, keepdims=True))
        weights = lax.optimization_barrier(jnp.exp(scores - row_max).astype(jnp.bfloat16)).astype(jnp.float32)
        attended = jnp.einsum('hqk,khd->qhd', weights, head_values)
        attended = attended * lax.rsqrt(lax.optimization_barrier(jnp.mean(attended * attended, axis=-1, keepdims=True)) + HEAD_FLOOR)
        return attended.reshape(TOK_A, HEADS * HD).astype(jnp.bfloat16)
    head_out = lax.map(attend_block, jnp.arange(N_EP, dtype=jnp.int32)).reshape(sequence, HEADS * HD)
    mixer_output = jnp.dot(head_out, output_weight, preferred_element_type=jnp.float32).astype(jnp.bfloat16)
    expert_normed = normed_rows(expert_tokens, expert_gain).reshape(N_EP, TOK_B, D)
    flat_routes = routes.reshape(N_EP, TOK_B * TOP)
    onehot = (flat_routes[:, :, None] == jnp.arange(EXPERTS, dtype=jnp.int32)[None, None, :]).astype(jnp.int32)
    slot_rank = lax.optimization_barrier(jnp.sum((jnp.cumsum(onehot, axis=1) - 1) * onehot, axis=2)).astype(jnp.int32)
    slot_index = flat_routes * CAP + slot_rank
    token_of = jnp.arange(TOK_B * TOP, dtype=jnp.int32) // TOP
    source = jnp.broadcast_to(jnp.arange(N_EP, dtype=jnp.int32)[:, None], flat_routes.shape)
    outgoing = jnp.zeros((N_EP, EXPERTS * CAP, D), jnp.bfloat16)
    outgoing = outgoing.at[source, slot_index].set(expert_normed[source, token_of[None, :]])
    groups = EXPERT_FF // N_TP

    def run_expert(number):
        slot_rows = lax.dynamic_slice_in_dim(outgoing, (number * CAP).astype(jnp.int32), CAP, 1)
        slot_rows = slot_rows.reshape(N_EP * CAP, D)
        gate_act = by_rows(slot_rows, gate_weight[number])
        up_act = by_rows(slot_rows, up_weight[number])
        hidden = (jax.nn.silu(gate_act) * up_act).astype(jnp.bfloat16)
        partial_value = jnp.einsum('rtf,tfd->trd', hidden.reshape(N_EP * CAP, N_TP, groups).astype(jnp.float32), down_weight[number].reshape(N_TP, groups, D).astype(jnp.float32))
        partial_value = lax.optimization_barrier(partial_value.astype(jnp.bfloat16)).astype(jnp.float32)
        return lax.optimization_barrier(jnp.sum(partial_value, axis=0)).astype(jnp.bfloat16)
    results = lax.map(run_expert, jnp.arange(EXPERTS, dtype=jnp.int32))
    picked = results.reshape(EXPERTS, N_EP, CAP, D)[flat_routes, source, slot_rank]
    weighted = picked.astype(jnp.float32) * route_weights.reshape(N_EP, TOK_B * TOP)[:, :, None]
    expert_output = lax.optimization_barrier(jnp.sum(weighted.reshape(N_EP, TOK_B, TOP, D), axis=2))
    expert_output = expert_output.reshape(N_EP * TOK_B, D).astype(jnp.bfloat16)
    return (mixer_output, expert_output)
```

```python
import jax
import jax.numpy as jnp
from jax import lax
from jax.experimental import pallas as pl
from jax.experimental.pallas import tpu as pltpu
from jax.sharding import Mesh
from jax.sharding import PartitionSpec as P

NZ, NX, NY, NC = 8, 4, 8, 2
HD = 64
ROWS_A = 192
ROWS_B = 128
D = 2048
FF = 224
CAP = 16
SLOTS = NZ * NX * CAP
QUART = 256
MEAN_FLOOR = 0.1
HEAD_FLOOR = 1.0
LOW = -1e30
MESH = pl.DeviceIdType.MESH
TP = ("y", "c")
EP = ("z", "x")
NEAR = (0, 1, 7, 2, 6, 3, 5, 4)
f32, bf16 = jnp.float32, jnp.bfloat16


def by_rows(left, right):
    return lax.dot_general(left, right, (((1,), (1,)), ((), ())), preferred_element_type=f32)


def exact(left, right):
    return jnp.dot(left, right, precision=lax.Precision.HIGHEST, preferred_element_type=f32)


def iota(shape, dim):
    return lax.broadcasted_iota(jnp.int32, shape, dim)


def rcopy(src, dst, send, recv, **where):
    return pltpu.make_async_remote_copy(
        src_ref=src,
        dst_ref=dst,
        send_sem=send,
        recv_sem=recv,
        device_id=where,
        device_id_type=MESH,
    )


def kernel(
    mt, mg, qw, kw, vw, fw, fb, ow, et, eg, rt, rw, gw_h, uw_h, dw_h,
    mo, eo,
    gw, uw, dw, dwp, w4, an, en, outrows, dispatch, comb,
    xm, xo, gacc, uacc, hid, hidp, pb, sbp, sbm, rbp, rbm, fin, res,
    qbuf, kvbuf, gmb, gx, gadj, gz, bias, po, pr, hbm, hbo, bw,
    lsem, ssem, dsem, ysem, psem, rsp, rsm, msem,
):
    z, x, y, c = (lax.axis_index(n) for n in ("z", "x", "y", "c"))
    other = 1 - c

    local = [
        pltpu.make_async_copy(gw_h.at[0], gw, lsem.at[0]),
        pltpu.make_async_copy(uw_h.at[0], uw, lsem.at[1]),
        pltpu.make_async_copy(dw_h.at[0], dw, lsem.at[2]),
        pltpu.make_async_copy(kw, w4.at[pl.ds(0, HD)], lsem.at[3]),
        pltpu.make_async_copy(vw, w4.at[pl.ds(HD, HD)], lsem.at[4]),
        pltpu.make_async_copy(qw, w4.at[pl.ds(2 * HD, HD)], lsem.at[5]),
    ]
    for cp in local:
        cp.start()

    barrier = pltpu.get_barrier_semaphore()
    for dz in range(NZ):
        for dx in range(NX):
            if dz or dx:
                pl.semaphore_signal(
                    barrier,
                    inc=1,
                    device_id={"z": lax.rem(z + dz, NZ), "x": lax.rem(x + dx, NX)},
                    device_id_type=MESH,
                )
    for dy in range(1, NY):
        pl.semaphore_signal(
            barrier, inc=1, device_id={"y": lax.rem(y + dy, NY)}, device_id_type=MESH
        )
    pl.semaphore_signal(barrier, inc=1, device_id={"c": other}, device_id_type=MESH)

    lane0 = pl.multiple_of((lax.rem(y, 4) * 2 + c) * QUART, QUART)

    def norm_b(i, _):
        rows = pl.ds(pl.multiple_of(i * 16, 16), 16)
        v = et[rows, :].astype(f32)
        sq = jnp.mean(v * v, axis=-1, keepdims=True)
        part = et[rows, pl.ds(lane0, QUART)].astype(f32)
        scaled = part * lax.rsqrt(jnp.maximum(sq, MEAN_FLOOR)) * eg[:, pl.ds(lane0, QUART)]
        en[rows, :] = scaled.astype(bf16)
        return 0

    lax.fori_loop(0, ROWS_B // 16, norm_b, 0)

    eid = iota((32, ROWS_B), 0)
    first = (eid == rt[0:1, :]).astype(f32)
    second = (eid == rt[1:2, :]).astype(f32)
    named = first + second
    before = (iota((ROWS_B, ROWS_B), 0) < iota((ROWS_B, ROWS_B), 1)).astype(bf16)
    rank = jnp.dot(named.astype(bf16), before, preferred_element_type=f32)
    rank = jnp.where(named > 0.5, rank, -1.0)
    pick = (lax.div(iota((SLOTS, 32), 0), CAP) == iota((SLOTS, 32), 1)).astype(f32)
    wide = jnp.dot(pick.astype(bf16), rank.astype(bf16), preferred_element_type=f32)
    chosen = wide == lax.rem(iota((SLOTS, ROWS_B), 0), CAP).astype(f32)
    dispatch[...] = chosen.astype(f32).astype(bf16)
    outrows[...] = jnp.dot(dispatch[...], en[...], preferred_element_type=f32).astype(bf16)

    pl.semaphore_wait(barrier, NZ * NX - 1 + NY - 1 + 1)

    local[2].wait()
    dwcopy = rcopy(dw, dwp, ssem.at[0], msem.at[0], c=other)
    dwcopy.start()
    mine = pl.multiple_of((z * NX + x) * CAP, CAP)
    for p, dzs in enumerate(NEAR):
        for dxs in range(NX):
            if dzs == 0 and dxs == 0:
                continue
            zt, xt = lax.rem(z + (NZ - dzs), NZ), lax.rem(x + (NX - dxs), NX)
            rcopy(
                outrows.at[pl.ds(pl.multiple_of((zt * NX + xt) * CAP, CAP), CAP)],
                xm.at[0, pl.ds((p * NX + dxs) * CAP, CAP)],
                ssem.at[1],
                dsem.at[p // 2],
                z=zt,
                x=xt,
            ).start()
    xm[0, 0:CAP, :] = outrows[pl.ds(mine, CAP), :]

    def norm_a(i, _):
        rows = pl.ds(pl.multiple_of(i * 16, 16), 16)
        v = mt[rows, :].astype(f32)
        sq = jnp.mean(v * v, axis=-1, keepdims=True)
        an[rows, :] = (v * lax.rsqrt(jnp.maximum(sq, MEAN_FLOOR)) * mg[...]).astype(bf16)
        return 0

    lax.fori_loop(0, ROWS_A // 16, norm_a, 0)
    w4[3 * HD : 4 * HD, :] = jnp.zeros((HD, D), bf16)
    for cp in local[3:6]:
        cp.wait()
    kvbuf[0:ROWS_A, :] = by_rows(an[...], w4[0 : 2 * HD, :]).astype(bf16)
    qs = by_rows(an[...], w4[2 * HD : 4 * HD, :]).astype(bf16) * jnp.asarray(HD**-0.5, bf16)
    qbuf[0:ROWS_A, :] = qs
    pre = by_rows(fw[...], an[...]) + fb[...]
    log_gate = jnp.minimum(pre, 0.0) - jnp.log1p(jnp.exp(-jnp.abs(pre)))
    upto = (iota((ROWS_A, 256), 0) <= iota((ROWS_A, 256), 1)).astype(f32)
    gmb[...] = exact(jnp.broadcast_to(log_gate, (8, ROWS_A)), upto)
    for dx in range(1, NX):
        xt = lax.rem(x + dx, NX)
        rcopy(gmb, gx.at[NX - dx], ssem.at[2], msem.at[1], x=xt).start()
        rcopy(
            qbuf.at[pl.ds(0, ROWS_A)],
            qbuf.at[pl.ds((NX - dx) * ROWS_A, ROWS_A)],
            ssem.at[3],
            msem.at[2],
            x=xt,
        ).start()
    for dz in range(1, NZ):
        rcopy(
            kvbuf.at[pl.ds(0, ROWS_A)],
            kvbuf.at[pl.ds((NZ - dz) * ROWS_A, ROWS_A)],
            ssem.at[4],
            msem.at[3],
            z=lax.rem(z + dz, NZ),
        ).start()
    gx0 = gx.at[pl.ds(1, NX - 1)]
    rcopy(gx0, gx0, ssem.at[2], msem.at[1], x=x).wait_recv()
    ahead = jnp.zeros((8, 1), f32)
    total = gmb[:, 255:256]
    for k in range(1, NX):
        t = gx[k, :, 255:256]
        ahead = ahead + t * (lax.rem(x + k, NX) < x).astype(f32)
        total = total + t
    gadj[...] = jnp.where(iota((8, 256), 1) < ROWS_A, gmb[...] + ahead, total)
    for dz in range(1, NZ):
        rcopy(gadj, gz.at[NZ - dz], ssem.at[5], msem.at[4], z=lax.rem(z + dz, NZ)).start()

    up, down = lax.rem(y + 1, NY), lax.rem(y + NY - 1, NY)
    up2, down2 = lax.rem(y + 2, NY), lax.rem(y + NY - 2, NY)
    for g in range(4):
        skip = CAP if g == 0 else 0
        got = xm.at[0, pl.ds(g * 128 + skip, 128 - skip)]
        rcopy(got, got, ssem.at[1], dsem.at[g], c=other).wait_recv()
        piece = pl.ds(g * 128, 128)
        src = xm.at[0, piece]
        rcopy(src, xm.at[3, piece], ssem.at[6], ysem.at[3], y=up).start()
        rcopy(src, xm.at[1, piece], ssem.at[7], ysem.at[1], y=down).start()
        rcopy(src, xm.at[2, piece], ssem.at[8], ysem.at[2], y=up2 if g < 2 else down2).start()
        rcopy(src, xo.at[0, piece], ssem.at[9], psem.at[0], c=other).start()

    weights = first * rw[0:1, :] + second * rw[1:2, :]
    spread = exact(pick, weights)
    comb[...] = jnp.where(dispatch[...] > 0.5, spread, 0.0).T
    bw[...] = jnp.zeros_like(bw)
    for h in range(16):
        bw[h * 128 : h * 128 + HD, 0:128] = ow[h * HD : (h + 1) * HD, :]
        bw[h * 128 + HD : h * 128 + 128, 128:256] = ow[h * HD : (h + 1) * HD, :]

    gz0 = gz.at[pl.ds(1, NZ - 1)]
    rcopy(gz0, gz0, ssem.at[5], msem.at[4], z=z).wait_recv()
    bias[...] = jnp.full((8, NZ * ROWS_A), LOW, f32)
    bias[:, 0:ROWS_A] = -gadj[:, 0:ROWS_A]
    back = jnp.zeros((8, 1), f32)
    for k in range(1, NZ):
        at = NZ - k
        back = back + gz[at, :, 255:256]
        bias[:, at * ROWS_A : (at + 1) * ROWS_A] = jnp.where(
            z - k >= 0, back - gz[at, :, 0:ROWS_A], LOW
        )
    q0 = qbuf.at[pl.ds(0, 3 * ROWS_A)]
    rcopy(q0, q0, ssem.at[3], msem.at[2], x=x).wait_recv()
    kv0 = kvbuf.at[pl.ds(0, 7 * ROWS_A)]
    rcopy(kv0, kv0, ssem.at[4], msem.at[3], z=z).wait_recv()
    HALF = ROWS_A // 2

    def attend(i, _):
        rows = pl.ds(pl.multiple_of(i * HALF, 32), HALF)
        dx = lax.div(i, 2)
        delta = (lax.rem(x + dx, NX) - x) * ROWS_A + lax.rem(i, 2) * HALF
        scores = by_rows(qbuf[rows, :], kvbuf[...]) + bias[0:1, :]
        lane = iota((HALF, 256), 1)
        seen = (lane <= iota((HALF, 256), 0) + delta) | (lane >= ROWS_A)
        scores = jnp.concatenate(
            [jnp.where(seen, scores[:, :256], LOW), scores[:, 256:]], axis=1
        )
        top = jnp.max(scores, axis=-1, keepdims=True)
        weight = jnp.exp(scores - top).astype(bf16)
        out = jnp.dot(weight, kvbuf[...], preferred_element_type=f32)
        po[rows, :] = jnp.where(iota((HALF, 128), 1) < HD, top, out)
        return 0

    lax.fori_loop(0, 2 * NX, attend, 0)
    for dx in range(1, NX):
        rcopy(
            po.at[pl.ds(dx * ROWS_A, ROWS_A)],
            pr.at[pl.ds((NX - dx) * ROWS_A, ROWS_A)],
            ssem.at[10],
            msem.at[5],
            x=lax.rem(x + dx, NX),
        ).start()

    local[0].wait()
    local[1].wait()

    def product(rows, k, core, start):
        cols = pl.ds(pl.multiple_of((lax.rem(y + k, 4) * 2 + core) * QUART, QUART), QUART)
        g, u = by_rows(rows, gw[:, cols]), by_rows(rows, uw[:, cols])
        if start:
            gacc[...], uacc[...] = g, u
        else:
            gacc[...] += g
            uacc[...] += u

    product(xm[0], 0, c, True)
    for k in (1, 3, 2):
        rcopy(xm.at[k], xm.at[k], ssem.at[6], ysem.at[k], y=up).wait_recv()
        rcopy(xm.at[k], xo.at[k], ssem.at[10 + k], psem.at[k], c=other).start()
        product(xm[k], k, c, False)
    for k in (0, 1, 3, 2):
        rcopy(xo.at[k], xo.at[k], ssem.at[9], psem.at[k], c=other).wait_recv()
        product(xo[k], k, other, False)
    gate = gacc[...]
    hid[...] = (gate * jax.nn.sigmoid(gate) * uacc[...]).astype(bf16)
    hcopy = rcopy(hid, hidp, ssem.at[14], msem.at[6], c=other)
    hcopy.start()
    dwcopy.wait_recv()
    hcopy.wait_recv()

    def down_block(j):
        cols = pl.ds(pl.multiple_of((lax.rem(y + j, NY) * 2 + c) * 128, 128), 128)
        pb[j] = jnp.dot(hid[...], dw[:, cols], preferred_element_type=f32) + jnp.dot(
            hidp[...], dwp[:, cols], preferred_element_type=f32
        )

    def plus(d, q, received):
        rows = pl.ds(q * 128, 128)
        v = pb[d, rows, :]
        if received:
            slot = rbp.at[d, rows]
            rcopy(slot, slot, ssem.at[15], rsp.at[d, q], y=up).wait_recv()
            v = v + rbp[d, rows, :].astype(f32)
        held = pl.ds(d * SLOTS + q * 128, 128)
        sbp[held, :] = v.astype(bf16)
        rcopy(
            sbp.at[held], rbp.at[d - 1, rows], ssem.at[15], rsp.at[d - 1, q], y=up
        ).start()

    def minus(d, q, received):
        rows = pl.ds(q * 128, 128)
        v = pb[NY - d, rows, :]
        if received:
            slot = rbm.at[d, rows]
            rcopy(slot, slot, ssem.at[16], rsm.at[d, q], y=down).wait_recv()
            v = v + rbm[d, rows, :].astype(f32)
        held = pl.ds(d * SLOTS + q * 128, 128)
        sbm[held, :] = v.astype(bf16)
        rcopy(
            sbm.at[held], rbm.at[d - 1, rows], ssem.at[16], rsm.at[d - 1, q], y=down
        ).start()

    down_block(4)
    for q in (0, 1):
        plus(4, q, False)
        minus(4, q + 2, False)
    down_block(3)
    down_block(5)
    for q in (0, 1):
        plus(3, q + 2, False)
        minus(3, q, False)
    for j in (2, 6, 1, 7, 0):
        down_block(j)
    for q in (0, 1):
        plus(3, q, True)
        minus(3, q + 2, True)
    for d in (2, 1):
        for q in (2, 3, 0, 1):
            plus(d, q, True)
            minus(d, (q + 2) % 4, True)

    pr0 = pr.at[pl.ds(0, 3 * ROWS_A)]
    rcopy(pr0, pr0, ssem.at[10], msem.at[5], x=x).wait_recv()
    parts = [po[0:ROWS_A, :]] + [pr[k * ROWS_A : (k + 1) * ROWS_A, :] for k in range(1, NX)]
    tops = [p[:, 0:1] for p in parts]
    top = jnp.maximum(jnp.maximum(tops[0], tops[1]), jnp.maximum(tops[2], tops[3]))
    att = sum(p * jnp.exp(t - top) for p, t in zip(parts, tops))
    att = jnp.where(iota((ROWS_A, 128), 1) < HD, 0.0, att)
    mean = jnp.sum(att * att, axis=-1, keepdims=True) * (1.0 / HD)
    head = att * lax.rsqrt(mean + HEAD_FLOOR)
    packed = jnp.where(
        iota((HALF, 128), 1) < HD, pltpu.roll(head[:HALF], HD, 1), head[HALF:]
    )
    hbm[pl.ds(y, 1)] = packed.astype(bf16)[None]
    for dy in range(1, NY):
        rcopy(hbm.at[y], hbm.at[y], ssem.at[17], msem.at[7], y=lax.rem(y + dy, NY)).start()

    for q in (0, 2, 1, 3):
        rows = pl.ds(q * 128, 128)
        ps, ms = rbp.at[0, rows], rbm.at[0, rows]
        rcopy(ps, ps, ssem.at[15], rsp.at[0, q], y=up).wait_recv()
        rcopy(ms, ms, ssem.at[16], rsm.at[0, q], y=down).wait_recv()
        v = pb[0, rows, :] + rbp[0, rows, :].astype(f32) + rbm[0, rows, :].astype(f32)
        fin[rows, :] = v.astype(bf16)
        for p in (2 * q, 2 * q + 1):
            for dxs in range(NX):
                at = pl.ds((p * NX + dxs) * CAP, CAP)
                if p == 0 and dxs == 0:
                    res[pl.ds(mine, CAP), :] = fin[0:CAP, :]
                    continue
                rcopy(
                    fin.at[at],
                    res.at[pl.ds(mine, CAP)],
                    ssem.at[18],
                    msem.at[8],
                    z=lax.rem(z + NEAR[p], NZ),
                    x=lax.rem(x + dxs, NX),
                ).start()

    h0 = hbm.at[pl.ds(0, NY - 1)]
    rcopy(h0, h0, ssem.at[17], msem.at[7], y=up).wait_recv()
    hc = rcopy(hbm, hbo, ssem.at[19], msem.at[9], c=other)
    hc.start()
    acc = jnp.zeros((HALF, 256), f32)
    for k in range(NY):
        acc = acc + jnp.dot(
            hbm[k], bw[pl.ds(pl.multiple_of((2 * k + c) * 128, 128), 128), :],
            preferred_element_type=f32,
        )
    hc.wait_recv()
    for k in range(NY):
        acc = acc + jnp.dot(
            hbo[k], bw[pl.ds(pl.multiple_of((2 * k + other) * 128, 128), 128), :],
            preferred_element_type=f32,
        )
    mo[0:HALF, :] = acc[:, 0:128].astype(bf16)
    mo[HALF:ROWS_A, :] = acc[:, 128:256].astype(bf16)

    r0 = res.at[pl.ds(0, SLOTS - CAP)]
    rcopy(r0, r0, ssem.at[18], msem.at[8], z=z).wait_recv()
    eo[...] = exact(comb[...], res[...].astype(f32)).astype(bf16)

    def sent(ref, sem):
        rcopy(ref, ref, ssem.at[sem], msem.at[0], c=other).wait_send()

    sent(dw, 0)
    sent(outrows.at[pl.ds(0, SLOTS - CAP)], 1)
    sent(gx.at[pl.ds(0, 3)], 2)
    sent(q0, 3)
    sent(kv0, 4)
    sent(gz0, 5)
    for s in (6, 7, 8, 9):
        sent(xm.at[0], s)
    sent(pr0, 10)
    for s in (11, 12, 13):
        sent(xm.at[0], s)
    sent(hid, 14)
    for s in (15, 16):
        sent(sbp.at[pl.ds(0, 14 * 128)], s)
    sent(h0, 17)
    sent(r0, 18)
    sent(hbm, 19)


def on_device(mt, mg, qw, kw, vw, fw, fb, ow, et, eg, rt, rw, gw, uw, dw):
    vmem = pl.BlockSpec(memory_space=pltpu.VMEM)
    hbm = pl.BlockSpec(memory_space=pl.ANY)
    dma = pltpu.SemaphoreType.DMA
    return pl.pallas_call(
        kernel,
        name="mixer_and_experts",
        out_shape=(
            jax.ShapeDtypeStruct((ROWS_A, 128), bf16),
            jax.ShapeDtypeStruct((ROWS_B, 128), bf16),
        ),
        in_specs=[vmem, vmem, hbm, hbm, hbm, vmem, vmem, vmem, vmem, vmem, vmem, vmem]
        + [hbm] * 3,
        out_specs=(vmem, vmem),
        scratch_shapes=[
            pltpu.VMEM((FF, D), bf16),
            pltpu.VMEM((FF, D), bf16),
            pltpu.VMEM((FF, D), bf16),
            pltpu.VMEM((FF, D), bf16),
            pltpu.VMEM((4 * HD, D), bf16),
            pltpu.VMEM((ROWS_A, D), bf16),
            pltpu.VMEM((ROWS_B, QUART), bf16),
            pltpu.VMEM((SLOTS, QUART), bf16),
            pltpu.VMEM((SLOTS, ROWS_B), bf16),
            pltpu.VMEM((ROWS_B, SLOTS), f32),
            pltpu.VMEM((4, SLOTS, QUART), bf16),
            pltpu.VMEM((4, SLOTS, QUART), bf16),
            pltpu.VMEM((SLOTS, FF), f32),
            pltpu.VMEM((SLOTS, FF), f32),
            pltpu.VMEM((SLOTS, FF), bf16),
            pltpu.VMEM((SLOTS, FF), bf16),
            pltpu.VMEM((NY, SLOTS, 128), f32),
            pltpu.VMEM((5 * SLOTS, 128), bf16),
            pltpu.VMEM((5 * SLOTS, 128), bf16),
            pltpu.VMEM((4, SLOTS, 128), bf16),
            pltpu.VMEM((4, SLOTS, 128), bf16),
            pltpu.VMEM((SLOTS, 128), bf16),
            pltpu.VMEM((SLOTS, 128), bf16),
            pltpu.VMEM((NX * ROWS_A, 128), bf16),
            pltpu.VMEM((NZ * ROWS_A, 128), bf16),
            pltpu.VMEM((8, 256), f32),
            pltpu.VMEM((NX, 8, 256), f32),
            pltpu.VMEM((8, 256), f32),
            pltpu.VMEM((NZ, 8, 256), f32),
            pltpu.VMEM((8, NZ * ROWS_A), f32),
            pltpu.VMEM((NX * ROWS_A, 128), f32),
            pltpu.VMEM((NX * ROWS_A, 128), f32),
            pltpu.VMEM((NY, ROWS_A // 2, 128), bf16),
            pltpu.VMEM((NY, ROWS_A // 2, 128), bf16),
            pltpu.VMEM((D, 256), bf16),
            dma((6,)),
            dma((20,)),
            dma((4,)),
            dma((4,)),
            dma((4,)),
            dma((4, 4)),
            dma((4, 4)),
            dma((10,)),
        ],
        compiler_params=pltpu.CompilerParams(collective_id=0, has_side_effects=True),
        cost_estimate=pl.CostEstimate(
            flops=3_000_000_000, bytes_accessed=6_000_000, transcendentals=1_200_000
        ),
    )(
        mt, mg.reshape(1, D), qw, kw, vw, fw.T, fb, ow, et, eg.reshape(1, D), rt.T, rw.T,
        gw, uw, dw,
    )


def solution(mesh):
    split = Mesh(mesh.devices.reshape(NZ, NX, NY, NC), ("z", "x", "y", "c"))
    return jax.shard_map(
        on_device,
        mesh=split,
        in_specs=(
            P(EP, None),
            P(),
            P(TP, None),
            P(TP, None),
            P(TP, None),
            P(None, TP),
            P(EP, TP),
            P(None, TP),
            P(EP, None),
            P(),
            P(EP, None),
            P(EP, None),
            P(EP, TP, None),
            P(EP, TP, None),
            P(EP, TP, None),
        ),
        out_specs=(P(EP, TP), P(EP, TP)),
        check_vma=False,
    )
```

```python
import jax
import jax.numpy as jnp
from jax import lax
from jax.experimental import pallas as pl
from jax.experimental.pallas import tpu as pltpu
from jax.sharding import Mesh
from jax.sharding import PartitionSpec as P

NZ, NX, NY, NC = 8, 4, 8, 2
HD = 64
ROWS_A = 192
ROWS_B = 128
D = 2048
FF = 224
CAP = 16
SLOTS = NZ * NX * CAP
QUART = 256
MEAN_FLOOR = 0.1
HEAD_FLOOR = 1.0
LOW = -1e30
MESH = pl.DeviceIdType.MESH
TP = ("y", "c")
EP = ("z", "x")
NEAR = (0, 1, 7, 2, 6, 3, 5, 4)
f32, bf16 = jnp.float32, jnp.bfloat16


def by_rows(left, right):
    return lax.dot_general(left, right, (((1,), (1,)), ((), ())), preferred_element_type=f32)


def exact(left, right):
    return jnp.dot(left, right, precision=lax.Precision.HIGHEST, preferred_element_type=f32)


def iota(shape, dim):
    return lax.broadcasted_iota(jnp.int32, shape, dim)


def rcopy(src, dst, send, recv, **where):
    return pltpu.make_async_remote_copy(
        src_ref=src,
        dst_ref=dst,
        send_sem=send,
        recv_sem=recv,
        device_id=where,
        device_id_type=MESH,
    )


def kernel(
    mt_h, mg_h, qw_h, kw_h, vw_h, fw_h, fb, ow_h, et_h, eg_h, rt_h, rw_h, gw_h, uw_h, dw_h,
    mo, eo,
    mt, mg, fw, ow, et, eg, rt, rw,
    gw, uw, dw, dwp, w4, an, en, outrows, dispatch, comb,
    xm, xo, gacc, uacc, hid, hidp, pb, sbp, sbm, rbp, rbm, fin, res,
    qbuf, kvbuf, gmb, gx, gadj, gz, bias, po, pr, hbm, hbo, bw,
    lsem, ssem, dsem, ysem, psem, rsp, rsm, msem,
):
    z, x, y, c = (lax.axis_index(n) for n in ("z", "x", "y", "c"))
    other = 1 - c

    local = [
        pltpu.make_async_copy(src, dst, lsem.at[i])
        for i, (src, dst) in enumerate(
            (
                (et_h, et),
                (eg_h, eg),
                (rt_h, rt),
                (rw_h, rw),
                (mt_h, mt),
                (mg_h, mg),
                (kw_h, w4.at[pl.ds(0, HD)]),
                (vw_h, w4.at[pl.ds(HD, HD)]),
                (qw_h, w4.at[pl.ds(2 * HD, HD)]),
                (fw_h, fw),
                (dw_h.at[0], dw),
                (gw_h.at[0], gw),
                (uw_h.at[0], uw),
                (ow_h, ow),
            )
        )
    ]
    for cp in local[:4]:
        cp.start()

    barrier = pltpu.get_barrier_semaphore()
    for dz in range(NZ):
        for dx in range(NX):
            if dz or dx:
                pl.semaphore_signal(
                    barrier,
                    inc=1,
                    device_id={"z": lax.rem(z + dz, NZ), "x": lax.rem(x + dx, NX)},
                    device_id_type=MESH,
                )
    for dy in range(1, NY):
        pl.semaphore_signal(
            barrier, inc=1, device_id={"y": lax.rem(y + dy, NY)}, device_id_type=MESH
        )
    pl.semaphore_signal(barrier, inc=1, device_id={"c": other}, device_id_type=MESH)
    for cp in local[4:]:
        cp.start()

    eid = iota((32, ROWS_B), 0)
    before = (iota((ROWS_B, ROWS_B), 0) < iota((ROWS_B, ROWS_B), 1)).astype(bf16)
    pick = (lax.div(iota((SLOTS, 32), 0), CAP) == iota((SLOTS, 32), 1)).astype(f32)
    for cp in local[:4]:
        cp.wait()
    first = (eid == rt[0:1, :]).astype(f32)
    second = (eid == rt[1:2, :]).astype(f32)
    named = first + second
    rank = jnp.dot(named.astype(bf16), before, preferred_element_type=f32)
    rank = jnp.where(named > 0.5, rank, -1.0)
    wide = jnp.dot(pick.astype(bf16), rank.astype(bf16), preferred_element_type=f32)
    chosen = wide == lax.rem(iota((SLOTS, ROWS_B), 0), CAP).astype(f32)
    dispatch[...] = chosen.astype(f32).astype(bf16)
    lane0 = pl.multiple_of((lax.rem(y, 4) * 2 + c) * QUART, QUART)

    def norm_b(i, _):
        rows = pl.ds(pl.multiple_of(i * 16, 16), 16)
        v = et[rows, :].astype(f32)
        sq = jnp.mean(v * v, axis=-1, keepdims=True)
        part = et[rows, pl.ds(lane0, QUART)].astype(f32)
        scaled = part * lax.rsqrt(jnp.maximum(sq, MEAN_FLOOR)) * eg[:, pl.ds(lane0, QUART)]
        en[rows, :] = scaled.astype(bf16)
        return 0

    lax.fori_loop(0, ROWS_B // 16, norm_b, 0, unroll=4)
    outrows[...] = jnp.dot(dispatch[...], en[...], preferred_element_type=f32).astype(bf16)

    pl.semaphore_wait(barrier, NZ * NX - 1 + NY - 1 + 1)

    mine = pl.multiple_of((z * NX + x) * CAP, CAP)
    for p, dzs in enumerate(NEAR):
        for dxs in range(NX):
            if dzs == 0 and dxs == 0:
                continue
            zt, xt = lax.rem(z + (NZ - dzs), NZ), lax.rem(x + (NX - dxs), NX)
            rcopy(
                outrows.at[pl.ds(pl.multiple_of((zt * NX + xt) * CAP, CAP), CAP)],
                xm.at[0, pl.ds((p * NX + dxs) * CAP, CAP)],
                ssem.at[1],
                dsem.at[p // 2],
                z=zt,
                x=xt,
            ).start()
    xm[0, 0:CAP, :] = outrows[pl.ds(mine, CAP), :]

    for cp in local[4:11]:
        cp.wait()
    dwcopy = rcopy(dw, dwp, ssem.at[0], msem.at[0], c=other)
    dwcopy.start()

    def norm_a(i, _):
        rows = pl.ds(pl.multiple_of(i * 16, 16), 16)
        v = mt[rows, :].astype(f32)
        sq = jnp.mean(v * v, axis=-1, keepdims=True)
        an[rows, :] = (v * lax.rsqrt(jnp.maximum(sq, MEAN_FLOOR)) * mg[...]).astype(bf16)
        return 0

    lax.fori_loop(0, ROWS_A // 16, norm_a, 0, unroll=4)
    w4[3 * HD : 4 * HD, :] = jnp.zeros((HD, D), bf16)
    pre = by_rows(fw[...], an[...]) + fb[...]
    log_gate = jnp.minimum(pre, 0.0) - jnp.log1p(jnp.exp(-jnp.abs(pre)))
    upto = (iota((ROWS_A, 256), 0) <= iota((ROWS_A, 256), 1)).astype(f32)
    gmb[...] = exact(jnp.broadcast_to(log_gate, (8, ROWS_A)), upto)
    for dx in range(1, NX):
        rcopy(gmb, gx.at[NX - dx], ssem.at[2], msem.at[1], x=lax.rem(x + dx, NX)).start()
    kvbuf[0:ROWS_A, :] = by_rows(an[...], w4[0 : 2 * HD, :]).astype(bf16)
    qs = by_rows(an[...], w4[2 * HD : 4 * HD, :]).astype(bf16) * jnp.asarray(HD**-0.5, bf16)
    qbuf[0:ROWS_A, :] = qs
    for dz in range(1, NZ):
        rcopy(
            kvbuf.at[pl.ds(0, ROWS_A)],
            kvbuf.at[pl.ds((NZ - dz) * ROWS_A, ROWS_A)],
            ssem.at[4],
            msem.at[3],
            z=lax.rem(z + dz, NZ),
        ).start()
    for dx in range(1, NX):
        rcopy(
            qbuf.at[pl.ds(0, ROWS_A)],
            qbuf.at[pl.ds((NX - dx) * ROWS_A, ROWS_A)],
            ssem.at[3],
            msem.at[2],
            x=lax.rem(x + dx, NX),
        ).start()

    up, down = lax.rem(y + 1, NY), lax.rem(y + NY - 1, NY)
    for g in range(4):
        skip = CAP if g == 0 else 0
        got = xm.at[0, pl.ds(g * 128 + skip, 128 - skip)]
        rcopy(got, got, ssem.at[1], dsem.at[g], c=other).wait_recv()
        piece = pl.ds(g * 128, 128)
        src = xm.at[0, piece]
        rcopy(src, xm.at[3, piece], ssem.at[6], ysem.at[3, g // 2], y=up).start()
        rcopy(src, xm.at[1, piece], ssem.at[7], ysem.at[1, g // 2], y=down).start()
        rcopy(src, xo.at[0, piece], ssem.at[9], psem.at[0], c=other).start()

    gx0 = gx.at[pl.ds(1, NX - 1)]
    rcopy(gx0, gx0, ssem.at[2], msem.at[1], x=x).wait_recv()
    ahead = jnp.zeros((8, 1), f32)
    total = gmb[:, 255:256]
    for k in range(1, NX):
        t = gx[k, :, 255:256]
        ahead = ahead + t * (lax.rem(x + k, NX) < x).astype(f32)
        total = total + t
    gadj[...] = jnp.where(iota((8, 256), 1) < ROWS_A, gmb[...] + ahead, total)
    for dz in range(1, NZ):
        rcopy(gadj, gz.at[NZ - dz], ssem.at[5], msem.at[4], z=lax.rem(z + dz, NZ)).start()

    for cp in local[11:]:
        cp.wait()

    def product(rows, k, core, start):
        cols = pl.ds(pl.multiple_of((lax.rem(y + k, 4) * 2 + core) * QUART, QUART), QUART)
        g, u = by_rows(rows, gw[:, cols]), by_rows(rows, uw[:, cols])
        if start:
            gacc[...], uacc[...] = g, u
        else:
            gacc[...] += g
            uacc[...] += u

    def arrived(k, h):
        half = xm.at[k, pl.ds(h * 256, 256)]
        rcopy(half, half, ssem.at[6], ysem.at[k, h], y=up).wait_recv()

    def to_partner(k):
        rcopy(xm.at[k], xo.at[k], ssem.at[10 + k], psem.at[k], c=other).start()

    def partner_product(k):
        rcopy(xo.at[k], xo.at[k], ssem.at[9], psem.at[k], c=other).wait_recv()
        product(xo[k], k, other, False)

    def relay(h):
        rows = pl.ds(h * 256, 256)
        arrived(3, h)
        src, dst = xm.at[3, rows, pl.ds(0, 128)], xm.at[2, rows, pl.ds(0, 128)]
        rcopy(src, dst, ssem.at[8], ysem.at[2, 0], y=up).start()
        arrived(1, h)
        src, dst = xm.at[1, rows, pl.ds(128, 128)], xm.at[2, rows, pl.ds(128, 128)]
        rcopy(src, dst, ssem.at[8], ysem.at[2, 0], y=down).start()

    product(xm[0], 0, c, True)
    relay(0)
    partner_product(0)
    relay(1)
    to_partner(3)
    to_partner(1)
    product(xm[3], 3, c, False)
    product(xm[1], 1, c, False)
    partner_product(3)
    partner_product(1)
    rcopy(xm.at[2], xm.at[2], ssem.at[6], ysem.at[2, 0], y=up).wait_recv()
    to_partner(2)
    product(xm[2], 2, c, False)
    partner_product(2)
    for h in range(2):
        rows = pl.ds(h * 256, 256)
        gate = gacc[rows, :]
        hid[rows, :] = (gate * jax.nn.sigmoid(gate) * uacc[rows, :]).astype(bf16)
        rcopy(hid.at[rows], hidp.at[rows], ssem.at[14], msem.at[6], c=other).start()

    def block(j, rows, weights):
        cols = pl.ds(pl.multiple_of((lax.rem(y + j, NY) * 2 + c) * 128, 128), 128)
        return jnp.dot(rows, weights[:, cols], preferred_element_type=f32)

    for j in (4, 3, 5, 2, 6, 1, 7, 0):
        pb[j] = block(j, hid[...], dw)
    dwcopy.wait_recv()
    rcopy(hid, hidp, ssem.at[14], msem.at[6], c=other).wait_recv()

    def plus(d, q, received):
        rows = pl.ds(q * 128, 128)
        v = pb[d, rows, :]
        if received:
            slot = rbp.at[d, rows]
            rcopy(slot, slot, ssem.at[15], rsp.at[d, q], y=up).wait_recv()
            v = v + rbp[d, rows, :].astype(f32)
        held = pl.ds(d * SLOTS + q * 128, 128)
        sbp[held, :] = v.astype(bf16)
        rcopy(
            sbp.at[held], rbp.at[d - 1, rows], ssem.at[15], rsp.at[d - 1, q], y=up
        ).start()

    def minus(d, q, received):
        rows = pl.ds(q * 128, 128)
        v = pb[NY - d, rows, :]
        if received:
            slot = rbm.at[d, rows]
            rcopy(slot, slot, ssem.at[16], rsm.at[d, q], y=down).wait_recv()
            v = v + rbm[d, rows, :].astype(f32)
        held = pl.ds(d * SLOTS + q * 128, 128)
        sbm[held, :] = v.astype(bf16)
        rcopy(
            sbm.at[held], rbm.at[d - 1, rows], ssem.at[16], rsm.at[d - 1, q], y=down
        ).start()

    HALF = ROWS_A // 2

    def attend(dx, half):
        rows = pl.ds(dx * ROWS_A + half * HALF, HALF)
        delta = (lax.rem(x + dx, NX) - x) * ROWS_A + half * HALF
        scores = by_rows(qbuf[rows, :], kvbuf[...]) + bias[0:1, :]
        lane = iota((HALF, 256), 1)
        seen = (lane <= iota((HALF, 256), 0) + delta) | (lane >= ROWS_A)
        scores = jnp.concatenate(
            [jnp.where(seen, scores[:, :256], LOW), scores[:, 256:]], axis=1
        )
        top = jnp.max(scores, axis=-1, keepdims=True)
        weight = jnp.exp(scores - top).astype(bf16)
        out = jnp.dot(weight, kvbuf[...], preferred_element_type=f32)
        po[rows, :] = jnp.where(iota((HALF, 128), 1) < HD, top, out)
        if half and dx:
            rcopy(
                po.at[pl.ds(dx * ROWS_A, ROWS_A)],
                pr.at[pl.ds((NX - dx) * ROWS_A, ROWS_A)],
                ssem.at[10],
                msem.at[5],
                x=lax.rem(x + dx, NX),
            ).start()

    pb[4] += block(4, hidp[...], dwp)
    for q in (0, 1):
        plus(4, q, False)
        minus(4, q + 2, False)
    for j in (3, 5):
        pb[j] += block(j, hidp[...], dwp)
    for q in (0, 1):
        plus(3, q + 2, False)
        minus(3, q, False)
    for j in (2, 6, 1, 7, 0):
        pb[j] += block(j, hidp[...], dwp)
    for q in (0, 1):
        plus(3, q, True)
        minus(3, q + 2, True)
    gz0 = gz.at[pl.ds(1, NZ - 1)]
    rcopy(gz0, gz0, ssem.at[5], msem.at[4], z=z).wait_recv()
    bias[:, 0:ROWS_A] = -gadj[:, 0:ROWS_A]
    back = jnp.zeros((8, 1), f32)
    for k in range(1, NZ):
        at = NZ - k
        back = back + gz[at, :, 255:256]
        bias[:, at * ROWS_A : (at + 1) * ROWS_A] = jnp.where(
            z - k >= 0, back - gz[at, :, 0:ROWS_A], LOW
        )
    q0 = qbuf.at[pl.ds(0, 3 * ROWS_A)]
    rcopy(q0, q0, ssem.at[3], msem.at[2], x=x).wait_recv()
    kv0 = kvbuf.at[pl.ds(0, 7 * ROWS_A)]
    rcopy(kv0, kv0, ssem.at[4], msem.at[3], z=z).wait_recv()
    order = [(2, 0), (2, 1), (1, 0), (1, 1), (3, 0), (3, 1), (0, 0), (0, 1)]
    for d in (2, 1):
        for q in (2, 3, 0, 1):
            plus(d, q, True)
            minus(d, (q + 2) % 4, True)
            attend(*order.pop(0))

    for q in (2, 0, 3, 1):
        rows = pl.ds(q * 128, 128)
        ps, ms = rbp.at[0, rows], rbm.at[0, rows]
        rcopy(ps, ps, ssem.at[15], rsp.at[0, q], y=up).wait_recv()
        rcopy(ms, ms, ssem.at[16], rsm.at[0, q], y=down).wait_recv()
        v = pb[0, rows, :] + rbp[0, rows, :].astype(f32) + rbm[0, rows, :].astype(f32)
        fin[rows, :] = v.astype(bf16)
        for p in (2 * q, 2 * q + 1):
            for dxs in range(NX):
                at = pl.ds((p * NX + dxs) * CAP, CAP)
                if p == 0 and dxs == 0:
                    res[pl.ds(mine, CAP), :] = fin[0:CAP, :]
                    continue
                rcopy(
                    fin.at[at],
                    res.at[pl.ds(mine, CAP)],
                    ssem.at[18],
                    msem.at[8],
                    z=lax.rem(z + NEAR[p], NZ),
                    x=lax.rem(x + dxs, NX),
                ).start()

    pr0 = pr.at[pl.ds(0, 3 * ROWS_A)]
    rcopy(pr0, pr0, ssem.at[10], msem.at[5], x=x).wait_recv()
    parts = [po[0:ROWS_A, :]] + [pr[k * ROWS_A : (k + 1) * ROWS_A, :] for k in range(1, NX)]
    tops = [p[:, 0:1] for p in parts]
    top = jnp.maximum(jnp.maximum(tops[0], tops[1]), jnp.maximum(tops[2], tops[3]))
    att = sum(p * jnp.exp(t - top) for p, t in zip(parts, tops))
    att = jnp.where(iota((ROWS_A, 128), 1) < HD, 0.0, att)
    mean = jnp.sum(att * att, axis=-1, keepdims=True) * (1.0 / HD)
    head = att * lax.rsqrt(mean + HEAD_FLOOR)
    packed = jnp.where(
        iota((HALF, 128), 1) < HD, pltpu.roll(head[:HALF], HD, 1), head[HALF:]
    )
    hbm[pl.ds(y, 1)] = packed.astype(bf16)[None]
    for dy in (4, 3, 5, 2, 6, 1, 7):
        rcopy(hbm.at[y], hbm.at[y], ssem.at[17], msem.at[7], y=lax.rem(y + dy, NY)).start()

    weights = first * rw[0:1, :] + second * rw[1:2, :]
    spread = exact(pick, weights)
    comb[...] = jnp.where(dispatch[...] > 0.5, spread, 0.0).T
    bw[...] = jnp.zeros_like(bw)
    for h in range(16):
        bw[h * 128 : h * 128 + HD, 0:128] = ow[h * HD : (h + 1) * HD, :]
        bw[h * 128 + HD : h * 128 + 128, 128:256] = ow[h * HD : (h + 1) * HD, :]

    h0 = hbm.at[pl.ds(0, NY - 1)]
    rcopy(h0, h0, ssem.at[17], msem.at[7], y=up).wait_recv()
    hc = rcopy(hbm, hbo, ssem.at[19], msem.at[9], c=other)
    hc.start()
    acc = jnp.zeros((HALF, 256), f32)
    for k in range(NY):
        acc = acc + jnp.dot(
            hbm[k], bw[pl.ds(pl.multiple_of((2 * k + c) * 128, 128), 128), :],
            preferred_element_type=f32,
        )

    r0 = res.at[pl.ds(0, SLOTS - CAP)]
    rcopy(r0, r0, ssem.at[18], msem.at[8], z=z).wait_recv()
    eo[...] = exact(comb[...], res[...].astype(f32)).astype(bf16)

    hc.wait_recv()
    for k in range(NY):
        acc = acc + jnp.dot(
            hbo[k], bw[pl.ds(pl.multiple_of((2 * k + other) * 128, 128), 128), :],
            preferred_element_type=f32,
        )
    mo[0:HALF, :] = acc[:, 0:128].astype(bf16)
    mo[HALF:ROWS_A, :] = acc[:, 128:256].astype(bf16)

    def sent(ref, sem):
        rcopy(ref, ref, ssem.at[sem], msem.at[0], c=other).wait_send()

    sent(dw, 0)
    sent(outrows.at[pl.ds(0, SLOTS - CAP)], 1)
    sent(gx0, 2)
    sent(q0, 3)
    sent(kv0, 4)
    sent(gz0, 5)
    for s in (6, 7, 8, 9):
        sent(xm.at[0], s)
    sent(pr0, 10)
    for s in (11, 12, 13):
        sent(xm.at[0], s)
    sent(hid, 14)
    for s in (15, 16):
        sent(sbp.at[pl.ds(0, 14 * 128)], s)
    sent(h0, 17)
    sent(r0, 18)
    sent(hbm, 19)


def on_device(mt, mg, qw, kw, vw, fw, fb, ow, et, eg, rt, rw, gw, uw, dw):
    vmem = pl.BlockSpec(memory_space=pltpu.VMEM)
    hbm = pl.BlockSpec(memory_space=pl.ANY)
    dma = pltpu.SemaphoreType.DMA
    return pl.pallas_call(
        kernel,
        name="mixer_and_experts",
        out_shape=(
            pltpu.VMEM((ROWS_A, 128), bf16),
            pltpu.VMEM((ROWS_B, 128), bf16),
        ),
        in_specs=[hbm] * 6 + [vmem] + [hbm] * 8,
        out_specs=(vmem, vmem),
        scratch_shapes=[
            pltpu.VMEM((ROWS_A, D), bf16),
            pltpu.VMEM((1, D), f32),
            pltpu.VMEM((1, D), bf16),
            pltpu.VMEM((16 * HD, 128), bf16),
            pltpu.VMEM((ROWS_B, D), bf16),
            pltpu.VMEM((1, D), f32),
            pltpu.VMEM((2, ROWS_B), jnp.int32),
            pltpu.VMEM((2, ROWS_B), f32),
            pltpu.VMEM((FF, D), bf16),
            pltpu.VMEM((FF, D), bf16),
            pltpu.VMEM((FF, D), bf16),
            pltpu.VMEM((FF, D), bf16),
            pltpu.VMEM((4 * HD, D), bf16),
            pltpu.VMEM((ROWS_A, D), bf16),
            pltpu.VMEM((ROWS_B, QUART), bf16),
            pltpu.VMEM((SLOTS, QUART), bf16),
            pltpu.VMEM((SLOTS, ROWS_B), bf16),
            pltpu.VMEM((ROWS_B, SLOTS), f32),
            pltpu.VMEM((4, SLOTS, QUART), bf16),
            pltpu.VMEM((4, SLOTS, QUART), bf16),
            pltpu.VMEM((SLOTS, FF), f32),
            pltpu.VMEM((SLOTS, FF), f32),
            pltpu.VMEM((SLOTS, FF), bf16),
            pltpu.VMEM((SLOTS, FF), bf16),
            pltpu.VMEM((NY, SLOTS, 128), f32),
            pltpu.VMEM((5 * SLOTS, 128), bf16),
            pltpu.VMEM((5 * SLOTS, 128), bf16),
            pltpu.VMEM((4, SLOTS, 128), bf16),
            pltpu.VMEM((4, SLOTS, 128), bf16),
            pltpu.VMEM((SLOTS, 128), bf16),
            pltpu.VMEM((SLOTS, 128), bf16),
            pltpu.VMEM((NX * ROWS_A, 128), bf16),
            pltpu.VMEM((NZ * ROWS_A, 128), bf16),
            pltpu.VMEM((8, 256), f32),
            pltpu.VMEM((NX, 8, 256), f32),
            pltpu.VMEM((8, 256), f32),
            pltpu.VMEM((NZ, 8, 256), f32),
            pltpu.VMEM((8, NZ * ROWS_A), f32),
            pltpu.VMEM((NX * ROWS_A, 128), f32),
            pltpu.VMEM((NX * ROWS_A, 128), f32),
            pltpu.VMEM((NY, ROWS_A // 2, 128), bf16),
            pltpu.VMEM((NY, ROWS_A // 2, 128), bf16),
            pltpu.VMEM((D, 256), bf16),
            dma((14,)),
            dma((20,)),
            dma((4,)),
            dma((4, 2)),
            dma((4,)),
            dma((4, 4)),
            dma((4, 4)),
            dma((10,)),
        ],
        compiler_params=pltpu.CompilerParams(collective_id=0, has_side_effects=True),
        cost_estimate=pl.CostEstimate(
            flops=3_000_000_000, bytes_accessed=6_000_000, transcendentals=1_200_000
        ),
    )(
        mt, mg.reshape(1, D), qw, kw, vw, fw.T, fb, ow, et, eg.reshape(1, D), rt.T, rw.T,
        gw, uw, dw,
    )


def solution(mesh):
    split = Mesh(mesh.devices.reshape(NZ, NX, NY, NC), ("z", "x", "y", "c"))
    return jax.shard_map(
        on_device,
        mesh=split,
        in_specs=(
            P(EP, None),
            P(),
            P(TP, None),
            P(TP, None),
            P(TP, None),
            P(None, TP),
            P(EP, TP),
            P(None, TP),
            P(EP, None),
            P(),
            P(EP, None),
            P(EP, None),
            P(EP, TP, None),
            P(EP, TP, None),
            P(EP, TP, None),
        ),
        out_specs=(P(EP, TP), P(EP, TP)),
        check_vma=False,
    )
```

```python
import jax
import jax.numpy as jnp
from jax import lax
from jax.experimental import pallas as pl
from jax.experimental.pallas import tpu as pltpu
from jax.sharding import Mesh
from jax.sharding import PartitionSpec as P

NZ, NX, NY, NC = 8, 4, 8, 2
HD = 64
ROWS_A = 192
ROWS_B = 128
D = 2048
FF = 224
CAP = 16
HALF = ROWS_A // 2
PIECE = (128, 128)
SLOTS = NZ * NX * CAP
QUART = 256
MEAN_FLOOR = 0.1
HEAD_FLOOR = 1.0
LOW = -1e30
MESH = pl.DeviceIdType.MESH
TP = ("y", "c")
EP = ("z", "x")
NEAR = (0, 1, 7, 2, 6, 3, 5, 4)
f32, bf16 = jnp.float32, jnp.bfloat16


def by_rows(left, right):
    return lax.dot_general(left, right, (((1,), (1,)), ((), ())), preferred_element_type=f32)


def exact(left, right):
    return jnp.dot(left, right, precision=lax.Precision.HIGHEST, preferred_element_type=f32)


def iota(shape, dim):
    return lax.broadcasted_iota(jnp.int32, shape, dim)


def rcopy(src, dst, send, recv, **where):
    return pltpu.make_async_remote_copy(
        src_ref=src,
        dst_ref=dst,
        send_sem=send,
        recv_sem=recv,
        device_id=where,
        device_id_type=MESH,
    )


def kernel(
    mt_h, mg_h, qw_h, kw_h, vw_h, fw_h, fb_h, ow_h, et_h, eg_h, rt_h, rw_h, gw_h, uw_h, dw_h,
    mo, eo,
    mt, mg, fw, fb, ow, et, eg, rt, rw,
    gw, uw, dw, dwp, w4, an, en, outrows, dispatch, comb,
    xm, xo, gacc, uacc, hid, hidp, pb, sbp, sbm, rbp, rbm, fin, res,
    qbuf, kvbuf, gmb, gx, gadj, gz, bias, sc, wt, po, pr, hbm, hbo, bw,
    lsem, ssem, dsem, ysem, psem, rsp, rsm, hsem, msem,
):
    z, x, y, c = (lax.axis_index(n) for n in ("z", "x", "y", "c"))
    other = 1 - c

    local = [
        pltpu.make_async_copy(src, dst, lsem.at[i])
        for i, (src, dst) in enumerate(
            (
                (et_h, et),
                (eg_h, eg),
                (rt_h, rt),
                (rw_h, rw),
                (mt_h, mt),
                (mg_h, mg),
                (kw_h, w4.at[pl.ds(0, HD)]),
                (vw_h, w4.at[pl.ds(HD, HD)]),
                (qw_h, w4.at[pl.ds(2 * HD, HD)]),
                (fw_h, fw),
                (fb_h, fb),
                (dw_h.at[0], dw),
                (gw_h.at[0], gw),
                (uw_h.at[0], uw),
                (ow_h, ow),
            )
        )
    ]
    for cp in local[:4]:
        cp.start()

    barrier = pltpu.get_barrier_semaphore()
    for dz in range(NZ):
        for dx in range(NX):
            if dz or dx:
                pl.semaphore_signal(
                    barrier,
                    inc=1,
                    device_id={"z": lax.rem(z + dz, NZ), "x": lax.rem(x + dx, NX)},
                    device_id_type=MESH,
                )
    for dy in range(1, NY):
        pl.semaphore_signal(
            barrier, inc=1, device_id={"y": lax.rem(y + dy, NY)}, device_id_type=MESH
        )
    pl.semaphore_signal(barrier, inc=1, device_id={"c": other}, device_id_type=MESH)
    for cp in local[4:]:
        cp.start()

    eid = iota((32, ROWS_B), 0)
    before = (iota((ROWS_B, ROWS_B), 0) < iota((ROWS_B, ROWS_B), 1)).astype(bf16)
    pick = (lax.div(iota((SLOTS, 32), 0), CAP) == iota((SLOTS, 32), 1)).astype(f32)
    for cp in local[:4]:
        cp.wait()
    first = (eid == rt[0:1, :]).astype(f32)
    second = (eid == rt[1:2, :]).astype(f32)
    named = first + second
    rank = jnp.dot(named.astype(bf16), before, preferred_element_type=f32)
    rank = jnp.where(named > 0.5, rank, -1.0)
    wide = jnp.dot(pick.astype(bf16), rank.astype(bf16), preferred_element_type=f32)
    chosen = wide == lax.rem(iota((SLOTS, ROWS_B), 0), CAP).astype(f32)
    dispatch[...] = chosen.astype(f32).astype(bf16)
    lane0 = pl.multiple_of((lax.rem(y, 4) * 2 + c) * QUART, QUART)

    def norm_b(i, _):
        rows = pl.ds(pl.multiple_of(i * 16, 16), 16)
        v = et[rows, :].astype(f32)
        sq = jnp.mean(v * v, axis=-1, keepdims=True)
        part = et[rows, pl.ds(lane0, QUART)].astype(f32)
        scaled = part * lax.rsqrt(jnp.maximum(sq, MEAN_FLOOR)) * eg[:, pl.ds(lane0, QUART)]
        en[rows, :] = scaled.astype(bf16)
        return 0

    lax.fori_loop(0, ROWS_B // 16, norm_b, 0, unroll=4)
    outrows[...] = jnp.dot(dispatch[...], en[...], preferred_element_type=f32).astype(bf16)

    pl.semaphore_wait(barrier, NZ * NX - 1 + NY - 1 + 1)

    mine = pl.multiple_of((z * NX + x) * CAP, CAP)
    for p, dzs in enumerate(NEAR):
        for dxs in range(NX):
            if dzs == 0 and dxs == 0:
                continue
            zt, xt = lax.rem(z + (NZ - dzs), NZ), lax.rem(x + (NX - dxs), NX)
            rcopy(
                outrows.at[pl.ds(pl.multiple_of((zt * NX + xt) * CAP, CAP), CAP)],
                xm.at[0, pl.ds((p * NX + dxs) * CAP, CAP)],
                ssem.at[1],
                dsem.at[p // 2],
                z=zt,
                x=xt,
            ).start()
    xm[0, 0:CAP, :] = outrows[pl.ds(mine, CAP), :]

    for cp in local[4:12]:
        cp.wait()
    dwcopy = rcopy(dw, dwp, ssem.at[0], msem.at[0], c=other)
    dwcopy.start()

    def norm_a(i, _):
        rows = pl.ds(pl.multiple_of(i * 16, 16), 16)
        v = mt[rows, :].astype(f32)
        sq = jnp.mean(v * v, axis=-1, keepdims=True)
        an[rows, :] = (v * lax.rsqrt(jnp.maximum(sq, MEAN_FLOOR)) * mg[...]).astype(bf16)
        return 0

    lax.fori_loop(0, ROWS_A // 16, norm_a, 0, unroll=4)
    w4[3 * HD : 4 * HD, :] = jnp.zeros((HD, D), bf16)
    pre = by_rows(fw[...], an[...]) + fb[...]
    log_gate = jnp.minimum(pre, 0.0) - jnp.log1p(jnp.exp(-jnp.abs(pre)))
    upto = (iota((ROWS_A, 256), 0) <= iota((ROWS_A, 256), 1)).astype(f32)
    gmb[...] = exact(jnp.broadcast_to(log_gate, (8, ROWS_A)), upto)
    for dx in range(1, NX):
        rcopy(gmb, gx.at[NX - dx], ssem.at[2], msem.at[1], x=lax.rem(x + dx, NX)).start()
    kvbuf[0:ROWS_A, :] = by_rows(an[...], w4[0 : 2 * HD, :]).astype(bf16)
    qs = by_rows(an[...], w4[2 * HD : 4 * HD, :]).astype(bf16) * jnp.asarray(HD**-0.5, bf16)
    qbuf[0:ROWS_A, :] = qs
    for dx in range(1, NX):
        rcopy(
            qbuf.at[pl.ds(0, ROWS_A)],
            qbuf.at[pl.ds((NX - dx) * ROWS_A, ROWS_A)],
            ssem.at[3],
            msem.at[2],
            x=lax.rem(x + dx, NX),
        ).start()

    up, down = lax.rem(y + 1, NY), lax.rem(y + NY - 1, NY)

    def spread_own(g):
        skip = CAP if g == 0 else 0
        got = xm.at[0, pl.ds(g * 128 + skip, 128 - skip)]
        rcopy(got, got, ssem.at[1], dsem.at[g], c=other).wait_recv()
        piece = pl.ds(g * 128, 128)
        src = xm.at[0, piece]
        rcopy(src, xm.at[3, piece], ssem.at[6], ysem.at[3, g], y=up).start()
        rcopy(src, xm.at[1, piece], ssem.at[7], ysem.at[1, g], y=down).start()
        rcopy(src, xo.at[0, piece], ssem.at[9], psem.at[0, g // 2], c=other).start()

    def product(h, src, k, core, start=False):
        rows = pl.ds(h * 256, 256)
        cols = pl.ds(pl.multiple_of((lax.rem(y + k, 4) * 2 + core) * QUART, QUART), QUART)
        v = src[k, rows, :]
        g, u = by_rows(v, gw[:, cols]), by_rows(v, uw[:, cols])
        if start:
            gacc[rows, :], uacc[rows, :] = g, u
        else:
            gacc[rows, :] += g
            uacc[rows, :] += u

    def arrived(k, g):
        piece = xm.at[k, pl.ds(g * 128, 128)]
        rcopy(piece, piece, ssem.at[6], ysem.at[k, g], y=up).wait_recv()

    def to_partner(k, at, count):
        rows = pl.ds(at, count)
        rcopy(
            xm.at[k, rows], xo.at[k, rows], ssem.at[10 + k], psem.at[k, at // 256], c=other
        ).start()

    def partner_product(h, k):
        got = xo.at[k, pl.ds(h * 256, 256)]
        rcopy(got, got, ssem.at[9], psem.at[k, h], c=other).wait_recv()
        product(h, xo, k, other)

    def relay(g):
        rows = pl.ds(g * 128, 128)
        for k, lane, to in ((3, 0, up), (1, 128, down)):
            arrived(k, g)
            rcopy(
                xm.at[k, rows, pl.ds(lane, 128)],
                xm.at[2, rows, pl.ds(lane, 128)],
                ssem.at[8],
                ysem.at[2, g],
                y=to,
            ).start()
            to_partner(k, g * 128, 128)

    def last_quarter(h):
        arrived(2, 2 * h)
        arrived(2, 2 * h + 1)
        to_partner(2, h * 256, 256)
        product(h, xm, 2, c)

    def block(j, rows, weights):
        cols = pl.ds(pl.multiple_of((lax.rem(y + j, NY) * 2 + c) * 128, 128), 128)
        return jnp.dot(rows, weights[:, cols], preferred_element_type=f32)

    BLOCKS = (4, 3, 5, 2, 6, 1, 7, 0)

    def hidden(h):
        partner_product(h, 2)
        rows = pl.ds(h * 256, 256)
        gate = gacc[rows, :]
        hid[rows, :] = (gate * jax.nn.sigmoid(gate) * uacc[rows, :]).astype(bf16)
        rcopy(hid.at[rows], hidp.at[rows], ssem.at[14], hsem.at[h], c=other).start()

    def own_blocks(h):
        rows = pl.ds(h * 256, 256)
        for j in BLOCKS:
            pb[j, rows, :] = block(j, hid[rows, :], dw)

    def hidden_arrived(h):
        got = hidp.at[pl.ds(h * 256, 256)]
        rcopy(got, got, ssem.at[14], hsem.at[h], c=other).wait_recv()

    def partner_blocks(h, which):
        rows = pl.ds(h * 256, 256)
        for j in which:
            pb[j, rows, :] += block(j, hidp[rows, :], dwp)

    spread_own(0)
    spread_own(1)
    for cp in local[12:]:
        cp.wait()
    product(0, xm, 0, c, True)
    spread_own(2)
    relay(0)
    spread_own(3)

    gx0 = gx.at[pl.ds(1, NX - 1)]
    rcopy(gx0, gx0, ssem.at[2], msem.at[1], x=x).wait_recv()
    ahead = jnp.zeros((8, 1), f32)
    total = gmb[:, 255:256]
    for k in range(1, NX):
        t = gx[k, :, 255:256]
        ahead = ahead + t * (lax.rem(x + k, NX) < x).astype(f32)
        total = total + t
    gadj[...] = jnp.where(iota((8, 256), 1) < ROWS_A, gmb[...] + ahead, total)
    for dz in range(1, NZ):
        rcopy(gadj, gz.at[NZ - dz], ssem.at[5], msem.at[4], z=lax.rem(z + dz, NZ)).start()
    for dz in range(1, NZ):
        rcopy(
            kvbuf.at[pl.ds(0, ROWS_A)],
            kvbuf.at[pl.ds((NZ - dz) * ROWS_A, ROWS_A)],
            ssem.at[4],
            msem.at[3],
            z=lax.rem(z + dz, NZ),
        ).start()

    relay(1)
    product(1, xm, 0, c, True)
    partner_product(0, 0)
    product(0, xm, 3, c)
    relay(2)
    product(0, xm, 1, c)
    partner_product(0, 3)
    partner_product(0, 1)
    relay(3)
    partner_product(1, 0)
    last_quarter(0)
    product(1, xm, 3, c)
    product(1, xm, 1, c)
    hidden(0)
    partner_product(1, 3)
    partner_product(1, 1)
    own_blocks(0)
    dwcopy.wait_recv()

    def onward(d, at, count, received, way):
        got, out, recv, to, sem, j = (
            (rbp, sbp, rsp, up, 15, d) if way else (rbm, sbm, rsm, down, 16, NY - d)
        )
        rows = pl.ds(at, count)
        v = pb[j, rows, :]
        if received:
            slot = got.at[d, rows]
            rcopy(slot, slot, ssem.at[sem], recv.at[d, at // 64], y=to).wait_recv()
            v = v + got[d, rows, :].astype(f32)
        held = pl.ds(d * SLOTS + at, count)
        out[held, :] = v.astype(bf16)
        rcopy(
            out.at[held], got.at[d - 1, rows], ssem.at[sem], recv.at[d - 1, at // 64], y=to
        ).start()

    def both(d, h, even, received):
        for i in range(0, 128, PIECE[h]):
            first = h * 256 + (0 if even else 128) + i
            second = h * 256 + (128 if even else 0) + i
            onward(d, first, PIECE[h], received, True)
            onward(d, second, PIECE[h], received, False)

    def scored(half):
        rows = pl.ds(half * 2 * ROWS_A, 2 * ROWS_A)
        sc[rows, :] = by_rows(qbuf[rows, :], kvbuf[...]) + bias[0:1, :]

    def weighed(dx):
        lane, row = iota((32, 256), 1), iota((32, 256), 0)
        for i in range(ROWS_A // 32):
            rows = pl.ds(dx * ROWS_A + i * 32, 32)
            delta = (lax.rem(x + dx, NX) - x) * ROWS_A + i * 32
            seen = (lane <= row + delta) | (lane >= ROWS_A)
            near = jnp.where(seen, sc[rows, 0:256], LOW)
            far = sc[rows, 256:]
            top = jnp.maximum(
                jnp.max(near, axis=-1, keepdims=True), jnp.max(far, axis=-1, keepdims=True)
            )
            wt[rows, 0:256] = jnp.exp(near - top).astype(bf16)
            wt[rows, 256:] = jnp.exp(far - top).astype(bf16)
            po[rows, :] = jnp.broadcast_to(top, (32, 128))

    def summed(half):
        rows = pl.ds(half * 2 * ROWS_A, 2 * ROWS_A)
        out = jnp.dot(wt[rows, :], kvbuf[...], preferred_element_type=f32)
        po[rows, :] = jnp.where(iota((2 * ROWS_A, 128), 1) < HD, po[rows, :], out)
        for dx in (2, 3) if half else (1,):
            rcopy(
                po.at[pl.ds(dx * ROWS_A, ROWS_A)],
                pr.at[pl.ds((NX - dx) * ROWS_A, ROWS_A)],
                ssem.at[10],
                msem.at[5],
                x=lax.rem(x + dx, NX),
            ).start()

    steps = [
        (scored, 1), (weighed, 2), (weighed, 3), (summed, 1),
        (scored, 0), (weighed, 1), (weighed, 0), (summed, 0),
    ]

    def attend(count):
        for _ in range(count):
            step, arg = steps.pop(0)
            step(arg)

    hidden_arrived(0)
    partner_blocks(0, (4,))
    both(4, 0, True, False)
    partner_blocks(0, (3, 5))
    both(3, 0, False, False)
    last_quarter(1)
    partner_blocks(0, (2, 6, 1, 7, 0))
    hidden(1)
    own_blocks(1)
    hidden_arrived(1)
    partner_blocks(1, (4,))
    both(4, 1, True, False)
    partner_blocks(1, (3, 5))
    both(3, 1, False, False)
    both(3, 0, True, True)
    both(2, 0, False, True)
    partner_blocks(1, (2, 6, 1, 7, 0))
    gz0 = gz.at[pl.ds(1, NZ - 1)]
    rcopy(gz0, gz0, ssem.at[5], msem.at[4], z=z).wait_recv()
    bias[:, 0:ROWS_A] = -gadj[:, 0:ROWS_A]
    back = jnp.zeros((8, 1), f32)
    for k in range(1, NZ):
        at = NZ - k
        back = back + gz[at, :, 255:256]
        bias[:, at * ROWS_A : (at + 1) * ROWS_A] = jnp.where(
            z - k >= 0, back - gz[at, :, 0:ROWS_A], LOW
        )
    q0 = qbuf.at[pl.ds(0, 3 * ROWS_A)]
    rcopy(q0, q0, ssem.at[3], msem.at[2], x=x).wait_recv()
    kv0 = kvbuf.at[pl.ds(0, 7 * ROWS_A)]
    rcopy(kv0, kv0, ssem.at[4], msem.at[3], z=z).wait_recv()
    attend(3)
    both(3, 1, True, True)
    both(2, 1, False, True)
    attend(1)
    both(2, 0, True, True)
    both(1, 0, False, True)
    attend(3)
    both(2, 1, True, True)
    both(1, 1, False, True)
    attend(1)
    both(1, 0, True, True)
    both(1, 1, True, True)

    def last(q):
        rows = pl.ds(q * 128, 128)
        piece = PIECE[q // 2]
        for at in range(q * 128, q * 128 + 128, piece):
            ps, ms = rbp.at[0, pl.ds(at, piece)], rbm.at[0, pl.ds(at, piece)]
            rcopy(ps, ps, ssem.at[15], rsp.at[0, at // 64], y=up).wait_recv()
            rcopy(ms, ms, ssem.at[16], rsm.at[0, at // 64], y=down).wait_recv()
        v = pb[0, rows, :] + rbp[0, rows, :].astype(f32) + rbm[0, rows, :].astype(f32)
        fin[rows, :] = v.astype(bf16)
        for p in (2 * q, 2 * q + 1):
            for dxs in range(NX):
                at = pl.ds((p * NX + dxs) * CAP, CAP)
                if p == 0 and dxs == 0:
                    res[pl.ds(mine, CAP), :] = fin[0:CAP, :]
                    continue
                rcopy(
                    fin.at[at],
                    res.at[pl.ds(mine, CAP)],
                    ssem.at[18],
                    msem.at[8],
                    z=lax.rem(z + NEAR[p], NZ),
                    x=lax.rem(x + dxs, NX),
                ).start()

    last(1)
    last(0)

    pr0 = pr.at[pl.ds(0, 3 * ROWS_A)]
    rcopy(pr0, pr0, ssem.at[10], msem.at[5], x=x).wait_recv()
    parts = [po[0:ROWS_A, :]] + [pr[k * ROWS_A : (k + 1) * ROWS_A, :] for k in range(1, NX)]
    tops = [p[:, 0:1] for p in parts]
    top = jnp.maximum(jnp.maximum(tops[0], tops[1]), jnp.maximum(tops[2], tops[3]))
    att = sum(p * jnp.exp(t - top) for p, t in zip(parts, tops))
    att = jnp.where(iota((ROWS_A, 128), 1) < HD, 0.0, att)
    mean = jnp.sum(att * att, axis=-1, keepdims=True) * (1.0 / HD)
    head = att * lax.rsqrt(mean + HEAD_FLOOR)
    packed = jnp.where(
        iota((HALF, 128), 1) < HD, pltpu.roll(head[:HALF], HD, 1), head[HALF:]
    )
    hbm[pl.ds(y, 1)] = packed.astype(bf16)[None]
    for dy in (4, 3, 5, 2, 6, 1, 7):
        rcopy(hbm.at[y], hbm.at[y], ssem.at[17], msem.at[7], y=lax.rem(y + dy, NY)).start()

    last(3)
    last(2)

    weights = first * rw[0:1, :] + second * rw[1:2, :]
    spread = exact(pick, weights)
    rest = jnp.where(dispatch[...] > 0.5, spread, 0.0).T
    for k in range(3):
        term = rest.astype(bf16)
        comb[k] = term
        rest = rest - term.astype(f32)
    bw[...] = jnp.zeros_like(bw)
    for h in range(16):
        bw[h * 128 : h * 128 + HD, 0:128] = ow[h * HD : (h + 1) * HD, :]
        bw[h * 128 + HD : h * 128 + 128, 128:256] = ow[h * HD : (h + 1) * HD, :]

    h0 = hbm.at[pl.ds(0, NY - 1)]
    rcopy(h0, h0, ssem.at[17], msem.at[7], y=up).wait_recv()
    hc = rcopy(hbm, hbo, ssem.at[19], msem.at[9], c=other)
    hc.start()
    acc = jnp.zeros((HALF, 256), f32)
    for k in range(NY):
        acc = acc + jnp.dot(
            hbm[k], bw[pl.ds(pl.multiple_of((2 * k + c) * 128, 128), 128), :],
            preferred_element_type=f32,
        )

    r0 = res.at[pl.ds(0, SLOTS - CAP)]
    rcopy(r0, r0, ssem.at[18], msem.at[8], z=z).wait_recv()
    eo[...] = sum(
        jnp.dot(comb[k], res[...], preferred_element_type=f32) for k in range(3)
    ).astype(bf16)

    hc.wait_recv()
    for k in range(NY):
        acc = acc + jnp.dot(
            hbo[k], bw[pl.ds(pl.multiple_of((2 * k + other) * 128, 128), 128), :],
            preferred_element_type=f32,
        )
    mo[0:HALF, :] = acc[:, 0:128].astype(bf16)
    mo[HALF:ROWS_A, :] = acc[:, 128:256].astype(bf16)

    def sent(ref, sem):
        rcopy(ref, ref, ssem.at[sem], msem.at[0], c=other).wait_send()

    sent(dw, 0)
    sent(outrows.at[pl.ds(0, SLOTS - CAP)], 1)
    sent(gx0, 2)
    sent(q0, 3)
    sent(kv0, 4)
    sent(gz0, 5)
    for s in (6, 7, 8, 9):
        sent(xm.at[0], s)
    sent(pr0, 10)
    for s in (11, 12, 13):
        sent(xm.at[0], s)
    sent(hid, 14)
    for s in (15, 16):
        sent(sbp.at[pl.ds(0, 14 * 128)], s)
    sent(h0, 17)
    sent(r0, 18)
    sent(hbm, 19)


def on_device(mt, mg, qw, kw, vw, fw, fb, ow, et, eg, rt, rw, gw, uw, dw):
    vmem = pl.BlockSpec(memory_space=pltpu.VMEM)
    hbm = pl.BlockSpec(memory_space=pl.ANY)
    dma = pltpu.SemaphoreType.DMA
    return pl.pallas_call(
        kernel,
        name="mixer_and_experts",
        out_shape=(
            pltpu.VMEM((ROWS_A, 128), bf16),
            pltpu.VMEM((ROWS_B, 128), bf16),
        ),
        in_specs=[hbm] * 15,
        out_specs=(vmem, vmem),
        scratch_shapes=[
            pltpu.VMEM((ROWS_A, D), bf16),
            pltpu.VMEM((1, D), f32),
            pltpu.VMEM((1, D), bf16),
            pltpu.VMEM((1, 1), f32),
            pltpu.VMEM((16 * HD, 128), bf16),
            pltpu.VMEM((ROWS_B, D), bf16),
            pltpu.VMEM((1, D), f32),
            pltpu.VMEM((2, ROWS_B), jnp.int32),
            pltpu.VMEM((2, ROWS_B), f32),
            pltpu.VMEM((FF, D), bf16),
            pltpu.VMEM((FF, D), bf16),
            pltpu.VMEM((FF, D), bf16),
            pltpu.VMEM((FF, D), bf16),
            pltpu.VMEM((4 * HD, D), bf16),
            pltpu.VMEM((ROWS_A, D), bf16),
            pltpu.VMEM((ROWS_B, QUART), bf16),
            pltpu.VMEM((SLOTS, QUART), bf16),
            pltpu.VMEM((SLOTS, ROWS_B), bf16),
            pltpu.VMEM((3, ROWS_B, SLOTS), bf16),
            pltpu.VMEM((4, SLOTS, QUART), bf16),
            pltpu.VMEM((4, SLOTS, QUART), bf16),
            pltpu.VMEM((SLOTS, FF), f32),
            pltpu.VMEM((SLOTS, FF), f32),
            pltpu.VMEM((SLOTS, FF), bf16),
            pltpu.VMEM((SLOTS, FF), bf16),
            pltpu.VMEM((NY, SLOTS, 128), f32),
            pltpu.VMEM((5 * SLOTS, 128), bf16),
            pltpu.VMEM((5 * SLOTS, 128), bf16),
            pltpu.VMEM((4, SLOTS, 128), bf16),
            pltpu.VMEM((4, SLOTS, 128), bf16),
            pltpu.VMEM((SLOTS, 128), bf16),
            pltpu.VMEM((SLOTS, 128), bf16),
            pltpu.VMEM((NX * ROWS_A, 128), bf16),
            pltpu.VMEM((NZ * ROWS_A, 128), bf16),
            pltpu.VMEM((8, 256), f32),
            pltpu.VMEM((NX, 8, 256), f32),
            pltpu.VMEM((8, 256), f32),
            pltpu.VMEM((NZ, 8, 256), f32),
            pltpu.VMEM((8, NZ * ROWS_A), f32),
            pltpu.VMEM((NX * ROWS_A, NZ * ROWS_A), f32),
            pltpu.VMEM((NX * ROWS_A, NZ * ROWS_A), bf16),
            pltpu.VMEM((NX * ROWS_A, 128), f32),
            pltpu.VMEM((NX * ROWS_A, 128), f32),
            pltpu.VMEM((NY, ROWS_A // 2, 128), bf16),
            pltpu.VMEM((NY, ROWS_A // 2, 128), bf16),
            pltpu.VMEM((D, 256), bf16),
            dma((15,)),
            dma((20,)),
            dma((4,)),
            dma((4, 4)),
            dma((4, 2)),
            dma((4, 8)),
            dma((4, 8)),
            dma((2,)),
            dma((10,)),
        ],
        compiler_params=pltpu.CompilerParams(collective_id=0, has_side_effects=True),
        cost_estimate=pl.CostEstimate(
            flops=3_000_000_000, bytes_accessed=6_000_000, transcendentals=1_200_000
        ),
    )(
        mt, mg.reshape(1, D), qw, kw, vw, fw.T, fb, ow, et, eg.reshape(1, D), rt.T, rw.T,
        gw, uw, dw,
    )


def solution(mesh):
    split = Mesh(mesh.devices.reshape(NZ, NX, NY, NC), ("z", "x", "y", "c"))
    return jax.shard_map(
        on_device,
        mesh=split,
        in_specs=(
            P(EP, None),
            P(),
            P(TP, None),
            P(TP, None),
            P(TP, None),
            P(None, TP),
            P(EP, TP),
            P(None, TP),
            P(EP, None),
            P(),
            P(EP, None),
            P(EP, None),
            P(EP, TP, None),
            P(EP, TP, None),
            P(EP, TP, None),
        ),
        out_specs=(P(EP, TP), P(EP, TP)),
        check_vma=False,
    )
```

```python
import jax
import jax.numpy as jnp
from jax import lax
from jax.experimental import pallas as pl
from jax.experimental.pallas import tpu as pltpu
from jax.sharding import Mesh
from jax.sharding import PartitionSpec as P

NZ, NX, NY, NC = 8, 4, 8, 2
HD = 64
ROWS_A = 192
ROWS_B = 128
D = 2048
FF = 224
CAP = 16
HALF = ROWS_A // 2
PIECE = (128, 128)
SLOTS = NZ * NX * CAP
QUART = 256
MEAN_FLOOR = 0.1
HEAD_FLOOR = 1.0
LOW = -1e30
MESH = pl.DeviceIdType.MESH
TP = ("y", "c")
EP = ("z", "x")
NEAR = (0, 1, 7, 2, 6, 3, 5, 4)
f32, bf16 = jnp.float32, jnp.bfloat16


def by_rows(left, right):
    return lax.dot_general(left, right, (((1,), (1,)), ((), ())), preferred_element_type=f32)


def exact(left, right):
    return jnp.dot(left, right, precision=lax.Precision.HIGHEST, preferred_element_type=f32)


def iota(shape, dim):
    return lax.broadcasted_iota(jnp.int32, shape, dim)


def rcopy(src, dst, send, recv, **where):
    return pltpu.make_async_remote_copy(
        src_ref=src,
        dst_ref=dst,
        send_sem=send,
        recv_sem=recv,
        device_id=where,
        device_id_type=MESH,
    )


def kernel(
    mt_h, mg_h, qw_h, kw_h, vw_h, fw_h, fb_h, ow_h, et_h, eg_h, rt_h, rw_h, gw_h, uw_h, dw_h,
    mo, eo,
    mt, mg, fw, fb, ow, et, eg, rt, rw,
    gw, uw, dw, dwp, w4, an, en, outrows, dispatch, comb,
    xm, xo, gacc, uacc, hid, hidp, pb, sbp, sbm, rbp, rbm, fin, res,
    qbuf, kvbuf, gmb, gx, gadj, gz, bias, sc, wt, po, pr, hbm, hbo, bw,
    lsem, ssem, dsem, ysem, psem, rsp, rsm, hsem, msem,
):
    z, x, y, c = (lax.axis_index(n) for n in ("z", "x", "y", "c"))
    other = 1 - c

    local = [
        pltpu.make_async_copy(src, dst, lsem.at[i])
        for i, (src, dst) in enumerate(
            (
                (et_h, et),
                (eg_h, eg),
                (rt_h, rt),
                (rw_h, rw),
                (mt_h, mt),
                (mg_h, mg),
                (kw_h, w4.at[pl.ds(0, HD)]),
                (vw_h, w4.at[pl.ds(HD, HD)]),
                (qw_h, w4.at[pl.ds(2 * HD, HD)]),
                (fw_h, fw),
                (fb_h, fb),
                (dw_h.at[0], dw),
                (gw_h.at[0], gw),
                (uw_h.at[0], uw),
                (ow_h, ow),
            )
        )
    ]
    for cp in (local[2], local[0], local[1], local[3]):
        cp.start()

    barrier = pltpu.get_barrier_semaphore()
    for dz in reversed(NEAR):
        for dx in (2, 1, 3, 0):
            if dz or dx:
                pl.semaphore_signal(
                    barrier,
                    inc=1,
                    device_id={"z": lax.rem(z + dz, NZ), "x": lax.rem(x + dx, NX)},
                    device_id_type=MESH,
                )
    for dy in NEAR[:0:-1]:
        pl.semaphore_signal(
            barrier, inc=1, device_id={"y": lax.rem(y + dy, NY)}, device_id_type=MESH
        )
    pl.semaphore_signal(barrier, inc=1, device_id={"c": other}, device_id_type=MESH)
    for cp in local[4:]:
        cp.start()

    eid = iota((32, ROWS_B), 0)
    before = (iota((ROWS_B, ROWS_B), 0) < iota((ROWS_B, ROWS_B), 1)).astype(bf16)
    pick = (lax.div(iota((SLOTS, 32), 0), CAP) == iota((SLOTS, 32), 1)).astype(f32)
    local[2].wait()
    first = (eid == rt[0:1, :]).astype(f32)
    second = (eid == rt[1:2, :]).astype(f32)
    named = first + second
    rank = jnp.dot(named.astype(bf16), before, preferred_element_type=f32)
    rank = jnp.where(named > 0.5, rank, -1.0)
    wide = jnp.dot(pick.astype(bf16), rank.astype(bf16), preferred_element_type=f32)
    chosen = wide == lax.rem(iota((SLOTS, ROWS_B), 0), CAP).astype(f32)
    dispatch[...] = chosen.astype(f32).astype(bf16)
    for cp in (local[0], local[1], local[3]):
        cp.wait()
    lane0 = pl.multiple_of((lax.rem(y, 4) * 2 + c) * QUART, QUART)

    def norm_b(i, _):
        rows = pl.ds(pl.multiple_of(i * 16, 16), 16)
        v = et[rows, :].astype(f32)
        sq = jnp.mean(v * v, axis=-1, keepdims=True)
        part = et[rows, pl.ds(lane0, QUART)].astype(f32)
        scaled = part * lax.rsqrt(jnp.maximum(sq, MEAN_FLOOR)) * eg[:, pl.ds(lane0, QUART)]
        en[rows, :] = scaled.astype(bf16)
        return 0

    lax.fori_loop(0, ROWS_B // 16, norm_b, 0, unroll=8)
    outrows[...] = jnp.dot(dispatch[...], en[...], preferred_element_type=f32).astype(bf16)

    pl.semaphore_wait(barrier, NZ * NX - 1 + NY - 1 + 1)

    mine = pl.multiple_of((z * NX + x) * CAP, CAP)
    for p, dzs in enumerate(NEAR):
        for dxs in range(NX):
            if dzs == 0 and dxs == 0:
                continue
            zt, xt = lax.rem(z + (NZ - dzs), NZ), lax.rem(x + (NX - dxs), NX)
            rcopy(
                outrows.at[pl.ds(pl.multiple_of((zt * NX + xt) * CAP, CAP), CAP)],
                xm.at[0, pl.ds((p * NX + dxs) * CAP, CAP)],
                ssem.at[1],
                dsem.at[p // 2],
                z=zt,
                x=xt,
            ).start()
    xm[0, 0:CAP, :] = outrows[pl.ds(mine, CAP), :]

    for cp in local[4:12]:
        cp.wait()
    dwcopy = rcopy(dw, dwp, ssem.at[0], msem.at[0], c=other)
    dwcopy.start()

    def norm_a(i, _):
        rows = pl.ds(pl.multiple_of(i * 16, 16), 16)
        v = mt[rows, :].astype(f32)
        sq = jnp.mean(v * v, axis=-1, keepdims=True)
        an[rows, :] = (v * lax.rsqrt(jnp.maximum(sq, MEAN_FLOOR)) * mg[...]).astype(bf16)
        return 0

    lax.fori_loop(0, ROWS_A // 16, norm_a, 0, unroll=4)
    w4[3 * HD : 4 * HD, :] = jnp.zeros((HD, D), bf16)
    pre = by_rows(fw[...], an[...]) + fb[...]
    log_gate = jnp.minimum(pre, 0.0) - jnp.log1p(jnp.exp(-jnp.abs(pre)))
    upto = (iota((ROWS_A, 256), 0) <= iota((ROWS_A, 256), 1)).astype(f32)
    gmb[...] = exact(jnp.broadcast_to(log_gate, (8, ROWS_A)), upto)
    for dx in range(1, NX):
        rcopy(gmb, gx.at[NX - dx], ssem.at[2], msem.at[1], x=lax.rem(x + dx, NX)).start()
    kvbuf[0:ROWS_A, :] = by_rows(an[...], w4[0 : 2 * HD, :]).astype(bf16)
    qs = by_rows(an[...], w4[2 * HD : 4 * HD, :]).astype(bf16) * jnp.asarray(HD**-0.5, bf16)
    qbuf[0:ROWS_A, :] = qs
    for dx in range(1, NX):
        rcopy(
            qbuf.at[pl.ds(0, ROWS_A)],
            qbuf.at[pl.ds((NX - dx) * ROWS_A, ROWS_A)],
            ssem.at[3],
            msem.at[2],
            x=lax.rem(x + dx, NX),
        ).start()

    up, down = lax.rem(y + 1, NY), lax.rem(y + NY - 1, NY)

    def spread_own(g):
        skip = CAP if g == 0 else 0
        got = xm.at[0, pl.ds(g * 128 + skip, 128 - skip)]
        rcopy(got, got, ssem.at[1], dsem.at[g], c=other).wait_recv()
        piece = pl.ds(g * 128, 128)
        src = xm.at[0, piece]
        rcopy(src, xm.at[3, piece], ssem.at[6], ysem.at[3, g], y=up).start()
        rcopy(src, xm.at[1, piece], ssem.at[7], ysem.at[1, g], y=down).start()
        rcopy(src, xo.at[0, piece], ssem.at[9], psem.at[0, g // 2], c=other).start()

    def product(h, src, k, core, start=False):
        rows = pl.ds(h * 256, 256)
        cols = pl.ds(pl.multiple_of((lax.rem(y + k, 4) * 2 + core) * QUART, QUART), QUART)
        v = src[k, rows, :]
        g, u = by_rows(v, gw[:, cols]), by_rows(v, uw[:, cols])
        if start:
            gacc[rows, :], uacc[rows, :] = g, u
        else:
            gacc[rows, :] += g
            uacc[rows, :] += u

    def arrived(k, g):
        piece = xm.at[k, pl.ds(g * 128, 128)]
        rcopy(piece, piece, ssem.at[6], ysem.at[k, g], y=up).wait_recv()

    def to_partner(k, at, count):
        rows = pl.ds(at, count)
        rcopy(
            xm.at[k, rows], xo.at[k, rows], ssem.at[10 + k], psem.at[k, at // 256], c=other
        ).start()

    def partner_product(h, k):
        got = xo.at[k, pl.ds(h * 256, 256)]
        rcopy(got, got, ssem.at[9], psem.at[k, h], c=other).wait_recv()
        product(h, xo, k, other)

    def relay(g):
        rows = pl.ds(g * 128, 128)
        for k, lane, to in ((3, 0, up), (1, 128, down)):
            arrived(k, g)
            rcopy(
                xm.at[k, rows, pl.ds(lane, 128)],
                xm.at[2, rows, pl.ds(lane, 128)],
                ssem.at[8],
                ysem.at[2, g],
                y=to,
            ).start()
            to_partner(k, g * 128, 128)

    def last_quarter(h):
        arrived(2, 2 * h)
        arrived(2, 2 * h + 1)
        to_partner(2, h * 256, 256)
        product(h, xm, 2, c)

    def block(j, rows, weights):
        cols = pl.ds(pl.multiple_of((lax.rem(y + j, NY) * 2 + c) * 128, 128), 128)
        return jnp.dot(rows, weights[:, cols], preferred_element_type=f32)

    BLOCKS = (4, 3, 5, 2, 6, 1, 7, 0)

    def hidden(h):
        partner_product(h, 2)
        rows = pl.ds(h * 256, 256)
        gate = gacc[rows, :]
        hid[rows, :] = (gate * jax.nn.sigmoid(gate) * uacc[rows, :]).astype(bf16)
        rcopy(hid.at[rows], hidp.at[rows], ssem.at[14], hsem.at[h], c=other).start()

    def own_blocks(h):
        rows = pl.ds(h * 256, 256)
        for j in BLOCKS:
            pb[j, rows, :] = block(j, hid[rows, :], dw)

    def hidden_arrived(h):
        got = hidp.at[pl.ds(h * 256, 256)]
        rcopy(got, got, ssem.at[14], hsem.at[h], c=other).wait_recv()

    def partner_blocks(h, which):
        rows = pl.ds(h * 256, 256)
        for j in which:
            pb[j, rows, :] += block(j, hidp[rows, :], dwp)

    spread_own(0)
    spread_own(1)
    for cp in local[12:]:
        cp.wait()
    product(0, xm, 0, c, True)
    spread_own(2)
    relay(0)
    spread_own(3)

    gx0 = gx.at[pl.ds(1, NX - 1)]
    rcopy(gx0, gx0, ssem.at[2], msem.at[1], x=x).wait_recv()
    ahead = jnp.zeros((8, 1), f32)
    total = gmb[:, 255:256]
    for k in range(1, NX):
        t = gx[k, :, 255:256]
        ahead = ahead + t * (lax.rem(x + k, NX) < x).astype(f32)
        total = total + t
    gadj[...] = jnp.where(iota((8, 256), 1) < ROWS_A, gmb[...] + ahead, total)
    for dz in range(1, NZ):
        rcopy(gadj, gz.at[NZ - dz], ssem.at[5], msem.at[4], z=lax.rem(z + dz, NZ)).start()
    for dz in range(1, NZ):
        rcopy(
            kvbuf.at[pl.ds(0, ROWS_A)],
            kvbuf.at[pl.ds((NZ - dz) * ROWS_A, ROWS_A)],
            ssem.at[4],
            msem.at[10],
            z=lax.rem(z + dz, NZ),
        ).start()

    relay(1)
    product(1, xm, 0, c, True)
    partner_product(0, 0)
    product(0, xm, 3, c)
    relay(2)
    product(0, xm, 1, c)
    partner_product(0, 3)
    partner_product(0, 1)
    relay(3)
    partner_product(1, 0)
    last_quarter(0)
    product(1, xm, 3, c)
    product(1, xm, 1, c)
    hidden(0)
    partner_product(1, 3)
    partner_product(1, 1)
    own_blocks(0)
    dwcopy.wait_recv()

    def onward(d, at, count, received, way):
        got, out, recv, to, sem, j = (
            (rbp, sbp, rsp, up, 15, d) if way else (rbm, sbm, rsm, down, 16, NY - d)
        )
        rows = pl.ds(at, count)
        v = pb[j, rows, :]
        if received:
            slot = got.at[d, rows]
            rcopy(slot, slot, ssem.at[sem], recv.at[d, at // 64], y=to).wait_recv()
            v = v + got[d, rows, :].astype(f32)
        held = pl.ds(d * SLOTS + at, count)
        out[held, :] = v.astype(bf16)
        rcopy(
            out.at[held], got.at[d - 1, rows], ssem.at[sem], recv.at[d - 1, at // 64], y=to
        ).start()

    def both(d, h, even, received):
        for i in range(0, 128, PIECE[h]):
            first = h * 256 + (0 if even else 128) + i
            second = h * 256 + (128 if even else 0) + i
            onward(d, first, PIECE[h], received, True)
            onward(d, second, PIECE[h], received, False)

    def scored(half):
        rows = pl.ds(half * 2 * ROWS_A, 2 * ROWS_A)
        sc[rows, :] = by_rows(qbuf[rows, :], kvbuf[...]) + bias[0:1, :]

    def weighed(dx):
        lane, row = iota((32, 256), 1), iota((32, 256), 0)
        for i in range(ROWS_A // 32):
            rows = pl.ds(dx * ROWS_A + i * 32, 32)
            delta = (lax.rem(x + dx, NX) - x) * ROWS_A + i * 32
            seen = (lane <= row + delta) | (lane >= ROWS_A)
            near = jnp.where(seen, sc[rows, 0:256], LOW)
            far = sc[rows, 256:]
            top = jnp.maximum(
                jnp.max(near, axis=-1, keepdims=True), jnp.max(far, axis=-1, keepdims=True)
            )
            wt[rows, 0:256] = jnp.exp(near - top).astype(bf16)
            wt[rows, 256:] = jnp.exp(far - top).astype(bf16)
            po[rows, :] = jnp.broadcast_to(top, (32, 128))

    def summed(half):
        rows = pl.ds(half * 2 * ROWS_A, 2 * ROWS_A)
        out = jnp.dot(wt[rows, :], kvbuf[...], preferred_element_type=f32)
        po[rows, :] = jnp.where(iota((2 * ROWS_A, 128), 1) < HD, po[rows, :], out)
        for dx in (2, 3) if half else (1,):
            rcopy(
                po.at[pl.ds(dx * ROWS_A, ROWS_A)],
                pr.at[pl.ds((NX - dx) * ROWS_A, ROWS_A)],
                ssem.at[10],
                msem.at[5],
                x=lax.rem(x + dx, NX),
            ).start()

    steps = [
        (scored, 1), (weighed, 2), (weighed, 3), (summed, 1),
        (scored, 0), (weighed, 1), (weighed, 0), (summed, 0),
    ]

    def attend(count):
        for _ in range(count):
            step, arg = steps.pop(0)
            step(arg)

    hidden_arrived(0)
    partner_blocks(0, (4,))
    both(4, 0, True, False)
    partner_blocks(0, (3, 5))
    both(3, 0, False, False)
    last_quarter(1)
    partner_blocks(0, (2, 6, 1, 7, 0))
    hidden(1)
    own_blocks(1)
    hidden_arrived(1)
    partner_blocks(1, (4,))
    both(4, 1, True, False)
    partner_blocks(1, (3, 5))
    both(3, 1, False, False)
    both(3, 0, True, True)
    both(2, 0, False, True)
    partner_blocks(1, (2, 6, 1, 7, 0))
    gz0 = gz.at[pl.ds(1, NZ - 1)]
    rcopy(gz0, gz0, ssem.at[5], msem.at[4], z=z).wait_recv()
    bias[:, 0:ROWS_A] = -gadj[:, 0:ROWS_A]
    back = jnp.zeros((8, 1), f32)
    for k in range(1, NZ):
        at = NZ - k
        back = back + gz[at, :, 255:256]
        bias[:, at * ROWS_A : (at + 1) * ROWS_A] = jnp.where(
            z - k >= 0, back - gz[at, :, 0:ROWS_A], LOW
        )
    q0 = qbuf.at[pl.ds(0, 3 * ROWS_A)]
    rcopy(q0, q0, ssem.at[3], msem.at[2], x=x).wait_recv()
    kv0 = kvbuf.at[pl.ds(0, 7 * ROWS_A)]
    rcopy(kv0, kv0, ssem.at[4], msem.at[10], z=z).wait_recv()
    attend(3)
    both(3, 1, True, True)
    both(2, 1, False, True)
    attend(1)
    both(2, 0, True, True)
    both(1, 0, False, True)
    attend(3)
    both(2, 1, True, True)
    both(1, 1, False, True)
    attend(1)
    both(1, 0, True, True)
    both(1, 1, True, True)

    def last(q):
        rows = pl.ds(q * 128, 128)
        piece = PIECE[q // 2]
        for at in range(q * 128, q * 128 + 128, piece):
            ps, ms = rbp.at[0, pl.ds(at, piece)], rbm.at[0, pl.ds(at, piece)]
            rcopy(ps, ps, ssem.at[15], rsp.at[0, at // 64], y=up).wait_recv()
            rcopy(ms, ms, ssem.at[16], rsm.at[0, at // 64], y=down).wait_recv()
        v = pb[0, rows, :] + rbp[0, rows, :].astype(f32) + rbm[0, rows, :].astype(f32)
        fin[rows, :] = v.astype(bf16)
        for p in (2 * q, 2 * q + 1):
            for dxs in range(NX):
                at = pl.ds((p * NX + dxs) * CAP, CAP)
                if p == 0 and dxs == 0:
                    res[pl.ds(mine, CAP), :] = fin[0:CAP, :]
                    continue
                rcopy(
                    fin.at[at],
                    res.at[pl.ds(mine, CAP)],
                    ssem.at[18],
                    msem.at[8],
                    z=lax.rem(z + NEAR[p], NZ),
                    x=lax.rem(x + dxs, NX),
                ).start()

    last(1)
    last(0)

    pr0 = pr.at[pl.ds(0, 3 * ROWS_A)]
    rcopy(pr0, pr0, ssem.at[10], msem.at[5], x=x).wait_recv()
    parts = [po[0:ROWS_A, :]] + [pr[k * ROWS_A : (k + 1) * ROWS_A, :] for k in range(1, NX)]
    tops = [p[:, 0:1] for p in parts]
    top = jnp.maximum(jnp.maximum(tops[0], tops[1]), jnp.maximum(tops[2], tops[3]))
    att = sum(p * jnp.exp(t - top) for p, t in zip(parts, tops))
    att = jnp.where(iota((ROWS_A, 128), 1) < HD, 0.0, att)
    mean = jnp.sum(att * att, axis=-1, keepdims=True) * (1.0 / HD)
    head = att * lax.rsqrt(mean + HEAD_FLOOR)
    packed = jnp.where(
        iota((HALF, 128), 1) < HD, pltpu.roll(head[:HALF], HD, 1), head[HALF:]
    )
    hbm[pl.ds(y, 1)] = packed.astype(bf16)[None]
    for dy in (4, 3, 5, 2, 6, 1, 7):
        rcopy(
            hbm.at[y],
            hbm.at[y],
            ssem.at[17],
            msem.at[7 if dy in (3, 4, 5) else 3],
            y=lax.rem(y + dy, NY),
        ).start()

    last(3)
    last(2)

    weights = first * rw[0:1, :] + second * rw[1:2, :]
    spread = exact(pick, weights)
    rest = jnp.where(dispatch[...] > 0.5, spread, 0.0).T
    for k in range(3):
        term = rest.astype(bf16)
        comb[k] = term
        rest = rest - term.astype(f32)
    bw[...] = jnp.zeros_like(bw)
    for h in range(16):
        bw[h * 128 : h * 128 + HD, 0:128] = ow[h * HD : (h + 1) * HD, :]
        bw[h * 128 + HD : h * 128 + 128, 128:256] = ow[h * HD : (h + 1) * HD, :]

    h0 = hbm.at[pl.ds(0, NY - 1)]
    hc = rcopy(hbm, hbo, ssem.at[19], msem.at[9], c=other)
    for sem, offsets in ((3, (0, 1, 7, 2, 6)), (7, (3, 5, 4))):
        some = hbm.at[pl.ds(0, 4 if sem == 3 else 3)]
        rcopy(some, some, ssem.at[17], msem.at[sem], y=up).wait_recv()
        for dy in offsets:
            at = lax.rem(y + dy, NY)
            rcopy(hbm.at[at], hbo.at[at], ssem.at[19], msem.at[9], c=other).start()
    acc = jnp.zeros((HALF, 256), f32)
    for k in range(NY):
        acc = acc + jnp.dot(
            hbm[k], bw[pl.ds(pl.multiple_of((2 * k + c) * 128, 128), 128), :],
            preferred_element_type=f32,
        )

    r0 = res.at[pl.ds(0, SLOTS - CAP)]

    def experts_out():
        rcopy(r0, r0, ssem.at[18], msem.at[8], z=z).wait_recv()
        eo[...] = sum(
            jnp.dot(comb[k], res[...], preferred_element_type=f32) for k in range(3)
        ).astype(bf16)

    def mixer_out():
        hc.wait_recv()
        whole = acc
        for k in range(NY):
            whole = whole + jnp.dot(
                hbo[k], bw[pl.ds(pl.multiple_of((2 * k + other) * 128, 128), 128), :],
                preferred_element_type=f32,
            )
        mo[0:HALF, :] = whole[:, 0:128].astype(bf16)
        mo[HALF:ROWS_A, :] = whole[:, 128:256].astype(bf16)

    @pl.when(c == 0)
    def _():
        mixer_out()
        experts_out()

    @pl.when(c == 1)
    def _():
        experts_out()
        mixer_out()

    def sent(ref, sem):
        rcopy(ref, ref, ssem.at[sem], msem.at[0], c=other).wait_send()

    sent(dw, 0)
    sent(outrows.at[pl.ds(0, SLOTS - CAP)], 1)
    sent(gx0, 2)
    sent(q0, 3)
    sent(kv0, 4)
    sent(gz0, 5)
    for s in (6, 7, 8, 9):
        sent(xm.at[0], s)
    sent(pr0, 10)
    for s in (11, 12, 13):
        sent(xm.at[0], s)
    sent(hid, 14)
    for s in (15, 16):
        sent(sbp.at[pl.ds(0, 14 * 128)], s)
    sent(h0, 17)
    sent(r0, 18)
    sent(hbm, 19)


def on_device(mt, mg, qw, kw, vw, fw, fb, ow, et, eg, rt, rw, gw, uw, dw):
    vmem = pl.BlockSpec(memory_space=pltpu.VMEM)
    hbm = pl.BlockSpec(memory_space=pl.ANY)
    dma = pltpu.SemaphoreType.DMA
    return pl.pallas_call(
        kernel,
        name="mixer_and_experts",
        out_shape=(
            pltpu.VMEM((ROWS_A, 128), bf16),
            pltpu.VMEM((ROWS_B, 128), bf16),
        ),
        in_specs=[hbm] * 15,
        out_specs=(vmem, vmem),
        scratch_shapes=[
            pltpu.VMEM((ROWS_A, D), bf16),
            pltpu.VMEM((1, D), f32),
            pltpu.VMEM((1, D), bf16),
            pltpu.VMEM((1, 1), f32),
            pltpu.VMEM((16 * HD, 128), bf16),
            pltpu.VMEM((ROWS_B, D), bf16),
            pltpu.VMEM((1, D), f32),
            pltpu.VMEM((2, ROWS_B), jnp.int32),
            pltpu.VMEM((2, ROWS_B), f32),
            pltpu.VMEM((FF, D), bf16),
            pltpu.VMEM((FF, D), bf16),
            pltpu.VMEM((FF, D), bf16),
            pltpu.VMEM((FF, D), bf16),
            pltpu.VMEM((4 * HD, D), bf16),
            pltpu.VMEM((ROWS_A, D), bf16),
            pltpu.VMEM((ROWS_B, QUART), bf16),
            pltpu.VMEM((SLOTS, QUART), bf16),
            pltpu.VMEM((SLOTS, ROWS_B), bf16),
            pltpu.VMEM((3, ROWS_B, SLOTS), bf16),
            pltpu.VMEM((4, SLOTS, QUART), bf16),
            pltpu.VMEM((4, SLOTS, QUART), bf16),
            pltpu.VMEM((SLOTS, FF), f32),
            pltpu.VMEM((SLOTS, FF), f32),
            pltpu.VMEM((SLOTS, FF), bf16),
            pltpu.VMEM((SLOTS, FF), bf16),
            pltpu.VMEM((NY, SLOTS, 128), f32),
            pltpu.VMEM((5 * SLOTS, 128), bf16),
            pltpu.VMEM((5 * SLOTS, 128), bf16),
            pltpu.VMEM((4, SLOTS, 128), bf16),
            pltpu.VMEM((4, SLOTS, 128), bf16),
            pltpu.VMEM((SLOTS, 128), bf16),
            pltpu.VMEM((SLOTS, 128), bf16),
            pltpu.VMEM((NX * ROWS_A, 128), bf16),
            pltpu.VMEM((NZ * ROWS_A, 128), bf16),
            pltpu.VMEM((8, 256), f32),
            pltpu.VMEM((NX, 8, 256), f32),
            pltpu.VMEM((8, 256), f32),
            pltpu.VMEM((NZ, 8, 256), f32),
            pltpu.VMEM((8, NZ * ROWS_A), f32),
            pltpu.VMEM((NX * ROWS_A, NZ * ROWS_A), f32),
            pltpu.VMEM((NX * ROWS_A, NZ * ROWS_A), bf16),
            pltpu.VMEM((NX * ROWS_A, 128), f32),
            pltpu.VMEM((NX * ROWS_A, 128), f32),
            pltpu.VMEM((NY, ROWS_A // 2, 128), bf16),
            pltpu.VMEM((NY, ROWS_A // 2, 128), bf16),
            pltpu.VMEM((D, 256), bf16),
            dma((15,)),
            dma((20,)),
            dma((4,)),
            dma((4, 4)),
            dma((4, 2)),
            dma((4, 8)),
            dma((4, 8)),
            dma((2,)),
            dma((11,)),
        ],
        compiler_params=pltpu.CompilerParams(collective_id=0, has_side_effects=True),
        cost_estimate=pl.CostEstimate(
            flops=3_000_000_000, bytes_accessed=6_000_000, transcendentals=1_200_000
        ),
    )(
        mt, mg.reshape(1, D), qw, kw, vw, fw.T, fb, ow, et, eg.reshape(1, D), rt.T, rw.T,
        gw, uw, dw,
    )


def solution(mesh):
    split = Mesh(mesh.devices.reshape(NZ, NX, NY, NC), ("z", "x", "y", "c"))
    return jax.shard_map(
        on_device,
        mesh=split,
        in_specs=(
            P(EP, None),
            P(),
            P(TP, None),
            P(TP, None),
            P(TP, None),
            P(None, TP),
            P(EP, TP),
            P(None, TP),
            P(EP, None),
            P(),
            P(EP, None),
            P(EP, None),
            P(EP, TP, None),
            P(EP, TP, None),
            P(EP, TP, None),
        ),
        out_specs=(P(EP, TP), P(EP, TP)),
        check_vma=False,
    )
```

```python
import jax
import jax.numpy as jnp
from jax import lax
from jax.experimental import pallas as pl
from jax.experimental.pallas import tpu as pltpu
from jax.sharding import Mesh
from jax.sharding import PartitionSpec as P

NZ, NX, NY, NC = 8, 4, 8, 2
HD = 64
ROWS_A = 192
ROWS_B = 128
D = 2048
FF = 224
CAP = 16
HALF = ROWS_A // 2
PIECE = (128, 128)
SLOTS = NZ * NX * CAP
QUART = 256
MEAN_FLOOR = 0.1
HEAD_FLOOR = 1.0
LOW = -1e30
MESH = pl.DeviceIdType.MESH
TP = ("y", "c")
EP = ("z", "x")
NEAR = (0, 1, 5, 4, 3, 6, 2, 7)
FAR_FIRST = (4, 3, 5, 2, 6, 1, 7, 0)
f32, bf16 = jnp.float32, jnp.bfloat16


def by_rows(left, right):
    return lax.dot_general(left, right, (((1,), (1,)), ((), ())), preferred_element_type=f32)


def exact(left, right):
    return jnp.dot(left, right, precision=lax.Precision.HIGHEST, preferred_element_type=f32)


def iota(shape, dim):
    return lax.broadcasted_iota(jnp.int32, shape, dim)


def rcopy(src, dst, send, recv, **where):
    return pltpu.make_async_remote_copy(
        src_ref=src,
        dst_ref=dst,
        send_sem=send,
        recv_sem=recv,
        device_id=where,
        device_id_type=MESH,
    )


def kernel(
    mt_h, mg_h, qw_h, kw_h, vw_h, fw_h, fb_h, ow_h, et_h, eg_h, rt_h, rw_h, gw_h, uw_h, dw_h,
    mo, eo,
    mt, mg, fw, fb, ow, et, eg, rt, rw,
    gw, uw, dw, dwp, w4, an, en, outrows, dispatch, comb,
    xm, xo, gacc, uacc, hid, hidp, pb, sbp, sbm, rbp, rbm, fin, res,
    qbuf, kvbuf, gmb, gx, gadj, gz, bias, sc, wt, po, pr, hbm, hbo, bw,
    lsem, ssem, dsem, ysem, psem, rsp, rsm, hsem, msem,
):
    z, x, y, c = (lax.axis_index(n) for n in ("z", "x", "y", "c"))
    other = 1 - c

    local = [
        pltpu.make_async_copy(src, dst, lsem.at[i])
        for i, (src, dst) in enumerate(
            (
                (et_h, et),
                (eg_h, eg),
                (rt_h, rt),
                (rw_h, rw),
                (mt_h, mt),
                (mg_h, mg),
                (kw_h, w4.at[pl.ds(0, HD)]),
                (vw_h, w4.at[pl.ds(HD, HD)]),
                (qw_h, w4.at[pl.ds(2 * HD, HD)]),
                (fw_h, fw),
                (fb_h, fb),
                (dw_h.at[0], dw),
                (gw_h.at[0], gw),
                (uw_h.at[0], uw),
                (ow_h, ow),
            )
        )
    ]
    for cp in (local[2], local[0], local[1], local[3]):
        cp.start()

    barrier = pltpu.get_barrier_semaphore()
    for dz in FAR_FIRST:
        for dx in (2, 1, 3, 0):
            if dz or dx:
                pl.semaphore_signal(
                    barrier,
                    inc=1,
                    device_id={"z": lax.rem(z + dz, NZ), "x": lax.rem(x + dx, NX)},
                    device_id_type=MESH,
                )
    for dy in FAR_FIRST[:-1]:
        pl.semaphore_signal(
            barrier, inc=1, device_id={"y": lax.rem(y + dy, NY)}, device_id_type=MESH
        )
    pl.semaphore_signal(barrier, inc=1, device_id={"c": other}, device_id_type=MESH)
    for cp in local[4:]:
        cp.start()

    eid = iota((32, ROWS_B), 0)
    before = (iota((ROWS_B, ROWS_B), 0) < iota((ROWS_B, ROWS_B), 1)).astype(bf16)
    pick = (lax.div(iota((SLOTS, 32), 0), CAP) == iota((SLOTS, 32), 1)).astype(f32)
    local[2].wait()
    first = (eid == rt[0:1, :]).astype(f32)
    second = (eid == rt[1:2, :]).astype(f32)
    named = first + second
    rank = jnp.dot(named.astype(bf16), before, preferred_element_type=f32)
    rank = jnp.where(named > 0.5, rank, -1.0)
    wide = jnp.dot(pick.astype(bf16), rank.astype(bf16), preferred_element_type=f32)
    chosen = wide == lax.rem(iota((SLOTS, ROWS_B), 0), CAP).astype(f32)
    dispatch[...] = chosen.astype(f32).astype(bf16)
    for cp in (local[0], local[1], local[3]):
        cp.wait()
    lane0 = pl.multiple_of((lax.rem(y, 4) * 2 + c) * QUART, QUART)

    def norm_b(i, _):
        rows = pl.ds(pl.multiple_of(i * 16, 16), 16)
        v = et[rows, :].astype(f32)
        sq = jnp.mean(v * v, axis=-1, keepdims=True)
        part = et[rows, pl.ds(lane0, QUART)].astype(f32)
        scaled = part * lax.rsqrt(jnp.maximum(sq, MEAN_FLOOR)) * eg[:, pl.ds(lane0, QUART)]
        en[rows, :] = scaled.astype(bf16)
        return 0

    lax.fori_loop(0, ROWS_B // 16, norm_b, 0, unroll=8)
    outrows[...] = jnp.dot(dispatch[...], en[...], preferred_element_type=f32).astype(bf16)

    pl.semaphore_wait(barrier, NZ * NX - 1 + NY - 1 + 1)

    mine = pl.multiple_of((z * NX + x) * CAP, CAP)
    for p, dzs in enumerate(NEAR):
        for dxs in range(NX):
            if dzs == 0 and dxs == 0:
                continue
            zt, xt = lax.rem(z + (NZ - dzs), NZ), lax.rem(x + (NX - dxs), NX)
            rcopy(
                outrows.at[pl.ds(pl.multiple_of((zt * NX + xt) * CAP, CAP), CAP)],
                xm.at[0, pl.ds((p * NX + dxs) * CAP, CAP)],
                ssem.at[1],
                dsem.at[p // 2],
                z=zt,
                x=xt,
            ).start()
    xm[0, 0:CAP, :] = outrows[pl.ds(mine, CAP), :]

    for cp in local[4:12]:
        cp.wait()
    dwcopy = rcopy(dw, dwp, ssem.at[0], msem.at[0], c=other)
    dwcopy.start()

    def norm_a(i, _):
        rows = pl.ds(pl.multiple_of(i * 16, 16), 16)
        v = mt[rows, :].astype(f32)
        sq = jnp.mean(v * v, axis=-1, keepdims=True)
        an[rows, :] = (v * lax.rsqrt(jnp.maximum(sq, MEAN_FLOOR)) * mg[...]).astype(bf16)
        return 0

    lax.fori_loop(0, ROWS_A // 16, norm_a, 0, unroll=4)
    w4[3 * HD : 4 * HD, :] = jnp.zeros((HD, D), bf16)
    pre = by_rows(fw[...], an[...]) + fb[...]
    log_gate = jnp.minimum(pre, 0.0) - jnp.log1p(jnp.exp(-jnp.abs(pre)))
    upto = (iota((ROWS_A, 256), 0) <= iota((ROWS_A, 256), 1)).astype(f32)
    gmb[...] = exact(jnp.broadcast_to(log_gate, (8, ROWS_A)), upto)
    for dx in range(1, NX):
        rcopy(gmb, gx.at[NX - dx], ssem.at[2], msem.at[1], x=lax.rem(x + dx, NX)).start()
    kvbuf[0:ROWS_A, :] = by_rows(an[...], w4[0 : 2 * HD, :]).astype(bf16)
    qs = by_rows(an[...], w4[2 * HD : 4 * HD, :]).astype(bf16) * jnp.asarray(HD**-0.5, bf16)
    qbuf[0:ROWS_A, :] = qs
    for dx in range(1, NX):
        rcopy(
            qbuf.at[pl.ds(0, ROWS_A)],
            qbuf.at[pl.ds((NX - dx) * ROWS_A, ROWS_A)],
            ssem.at[3],
            msem.at[2],
            x=lax.rem(x + dx, NX),
        ).start()

    up, down = lax.rem(y + 1, NY), lax.rem(y + NY - 1, NY)

    def spread_own(g):
        skip = CAP if g == 0 else 0
        got = xm.at[0, pl.ds(g * 128 + skip, 128 - skip)]
        rcopy(got, got, ssem.at[1], dsem.at[g], c=other).wait_recv()
        piece = pl.ds(g * 128, 128)
        src = xm.at[0, piece]
        rcopy(src, xm.at[3, piece], ssem.at[6], ysem.at[3, g], y=up).start()
        rcopy(src, xm.at[1, piece], ssem.at[7], ysem.at[1, g], y=down).start()
        rcopy(src, xo.at[0, piece], ssem.at[9], psem.at[0, g // 2], c=other).start()

    def product(h, src, k, core, start=False):
        rows = pl.ds(h * 256, 256)
        cols = pl.ds(pl.multiple_of((lax.rem(y + k, 4) * 2 + core) * QUART, QUART), QUART)
        v = src[k, rows, :]
        g, u = by_rows(v, gw[:, cols]), by_rows(v, uw[:, cols])
        if start:
            gacc[rows, :], uacc[rows, :] = g, u
        else:
            gacc[rows, :] += g
            uacc[rows, :] += u

    def arrived(k, g):
        piece = xm.at[k, pl.ds(g * 128, 128)]
        rcopy(piece, piece, ssem.at[6], ysem.at[k, g], y=up).wait_recv()

    def to_partner(k, at, count):
        rows = pl.ds(at, count)
        rcopy(
            xm.at[k, rows], xo.at[k, rows], ssem.at[10 + k], psem.at[k, at // 256], c=other
        ).start()

    def partner_product(h, k):
        got = xo.at[k, pl.ds(h * 256, 256)]
        rcopy(got, got, ssem.at[9], psem.at[k, h], c=other).wait_recv()
        product(h, xo, k, other)

    def relay(g):
        rows = pl.ds(g * 128, 128)
        for k, lane, to in ((3, 0, up), (1, 128, down)):
            arrived(k, g)
            rcopy(
                xm.at[k, rows, pl.ds(lane, 128)],
                xm.at[2, rows, pl.ds(lane, 128)],
                ssem.at[8],
                ysem.at[2, g],
                y=to,
            ).start()
            to_partner(k, g * 128, 128)

    def last_quarter(h):
        arrived(2, 2 * h)
        arrived(2, 2 * h + 1)
        to_partner(2, h * 256, 256)
        product(h, xm, 2, c)

    def block(j, rows, weights):
        cols = pl.ds(pl.multiple_of((lax.rem(y + j, NY) * 2 + c) * 128, 128), 128)
        return jnp.dot(rows, weights[:, cols], preferred_element_type=f32)

    BLOCKS = (4, 3, 5, 2, 6, 1, 7, 0)

    def hidden(h):
        partner_product(h, 2)
        rows = pl.ds(h * 256, 256)
        gate = gacc[rows, :]
        hid[rows, :] = (gate * jax.nn.sigmoid(gate) * uacc[rows, :]).astype(bf16)
        rcopy(hid.at[rows], hidp.at[rows], ssem.at[14], hsem.at[h], c=other).start()

    def own_blocks(h):
        rows = pl.ds(h * 256, 256)
        for j in BLOCKS:
            pb[j, rows, :] = block(j, hid[rows, :], dw)

    def hidden_arrived(h):
        got = hidp.at[pl.ds(h * 256, 256)]
        rcopy(got, got, ssem.at[14], hsem.at[h], c=other).wait_recv()

    def partner_blocks(h, which):
        rows = pl.ds(h * 256, 256)
        for j in which:
            pb[j, rows, :] += block(j, hidp[rows, :], dwp)

    spread_own(0)
    spread_own(1)
    for cp in local[12:]:
        cp.wait()
    product(0, xm, 0, c, True)
    spread_own(2)
    relay(0)
    spread_own(3)

    gx0 = gx.at[pl.ds(1, NX - 1)]
    rcopy(gx0, gx0, ssem.at[2], msem.at[1], x=x).wait_recv()
    ahead = jnp.zeros((8, 1), f32)
    total = gmb[:, 255:256]
    for k in range(1, NX):
        t = gx[k, :, 255:256]
        ahead = ahead + t * (lax.rem(x + k, NX) < x).astype(f32)
        total = total + t
    gadj[...] = jnp.where(iota((8, 256), 1) < ROWS_A, gmb[...] + ahead, total)
    for dz in range(1, NZ):
        rcopy(gadj, gz.at[NZ - dz], ssem.at[5], msem.at[4], z=lax.rem(z + dz, NZ)).start()
    for dz in range(1, NZ):
        rcopy(
            kvbuf.at[pl.ds(0, ROWS_A)],
            kvbuf.at[pl.ds((NZ - dz) * ROWS_A, ROWS_A)],
            ssem.at[4],
            msem.at[10],
            z=lax.rem(z + dz, NZ),
        ).start()

    relay(1)
    product(1, xm, 0, c, True)
    partner_product(0, 0)
    product(0, xm, 3, c)
    relay(2)
    product(0, xm, 1, c)
    partner_product(0, 3)
    partner_product(0, 1)
    relay(3)
    partner_product(1, 0)
    last_quarter(0)
    product(1, xm, 3, c)
    product(1, xm, 1, c)
    hidden(0)
    partner_product(1, 3)
    partner_product(1, 1)
    own_blocks(0)
    dwcopy.wait_recv()

    def onward(d, at, count, received, way):
        got, out, recv, to, sem, j = (
            (rbp, sbp, rsp, up, 15, d) if way else (rbm, sbm, rsm, down, 16, NY - d)
        )
        rows = pl.ds(at, count)
        v = pb[j, rows, :]
        if received:
            slot = got.at[d, rows]
            rcopy(slot, slot, ssem.at[sem], recv.at[d, at // 64], y=to).wait_recv()
            v = v + got[d, rows, :].astype(f32)
        held = pl.ds(d * SLOTS + at, count)
        out[held, :] = v.astype(bf16)
        rcopy(
            out.at[held], got.at[d - 1, rows], ssem.at[sem], recv.at[d - 1, at // 64], y=to
        ).start()

    def both(d, h, even, received):
        for i in range(0, 128, PIECE[h]):
            first = h * 256 + (0 if even else 128) + i
            second = h * 256 + (128 if even else 0) + i
            onward(d, first, PIECE[h], received, True)
            onward(d, second, PIECE[h], received, False)

    def scored(half):
        rows = pl.ds(half * 2 * ROWS_A, 2 * ROWS_A)
        sc[rows, :] = by_rows(qbuf[rows, :], kvbuf[...]) + bias[0:1, :]

    def weighed(dx):
        lane, row = iota((32, 256), 1), iota((32, 256), 0)
        for i in range(ROWS_A // 32):
            rows = pl.ds(dx * ROWS_A + i * 32, 32)
            delta = (lax.rem(x + dx, NX) - x) * ROWS_A + i * 32
            seen = (lane <= row + delta) | (lane >= ROWS_A)
            near = jnp.where(seen, sc[rows, 0:256], LOW)
            far = sc[rows, 256:]
            top = jnp.maximum(
                jnp.max(near, axis=-1, keepdims=True), jnp.max(far, axis=-1, keepdims=True)
            )
            wt[rows, 0:256] = jnp.exp(near - top).astype(bf16)
            wt[rows, 256:] = jnp.exp(far - top).astype(bf16)
            po[rows, :] = jnp.broadcast_to(top, (32, 128))

    def summed(half):
        rows = pl.ds(half * 2 * ROWS_A, 2 * ROWS_A)
        out = jnp.dot(wt[rows, :], kvbuf[...], preferred_element_type=f32)
        po[rows, :] = jnp.where(iota((2 * ROWS_A, 128), 1) < HD, po[rows, :], out)
        for dx in (2, 3) if half else (1,):
            rcopy(
                po.at[pl.ds(dx * ROWS_A, ROWS_A)],
                pr.at[pl.ds((NX - dx) * ROWS_A, ROWS_A)],
                ssem.at[10],
                msem.at[5],
                x=lax.rem(x + dx, NX),
            ).start()

    steps = [
        (scored, 1), (weighed, 2), (weighed, 3), (summed, 1),
        (scored, 0), (weighed, 1), (weighed, 0), (summed, 0),
    ]

    def attend(count):
        for _ in range(count):
            step, arg = steps.pop(0)
            step(arg)

    hidden_arrived(0)
    partner_blocks(0, (4,))
    both(4, 0, True, False)
    partner_blocks(0, (3, 5))
    both(3, 0, False, False)
    last_quarter(1)
    partner_blocks(0, (2, 6, 1, 7, 0))
    hidden(1)
    own_blocks(1)
    hidden_arrived(1)
    partner_blocks(1, (4,))
    both(4, 1, True, False)
    partner_blocks(1, (3, 5))
    both(3, 1, False, False)
    both(3, 0, True, True)
    both(2, 0, False, True)
    partner_blocks(1, (2, 6, 1, 7, 0))
    gz0 = gz.at[pl.ds(1, NZ - 1)]
    rcopy(gz0, gz0, ssem.at[5], msem.at[4], z=z).wait_recv()
    bias[:, 0:ROWS_A] = -gadj[:, 0:ROWS_A]
    back = jnp.zeros((8, 1), f32)
    for k in range(1, NZ):
        at = NZ - k
        back = back + gz[at, :, 255:256]
        bias[:, at * ROWS_A : (at + 1) * ROWS_A] = jnp.where(
            z - k >= 0, back - gz[at, :, 0:ROWS_A], LOW
        )
    q0 = qbuf.at[pl.ds(0, 3 * ROWS_A)]
    rcopy(q0, q0, ssem.at[3], msem.at[2], x=x).wait_recv()
    kv0 = kvbuf.at[pl.ds(0, 7 * ROWS_A)]
    rcopy(kv0, kv0, ssem.at[4], msem.at[10], z=z).wait_recv()
    attend(3)
    both(3, 1, True, True)
    both(2, 1, False, True)
    attend(1)
    both(2, 0, True, True)
    both(1, 0, False, True)
    attend(3)
    both(2, 1, True, True)
    both(1, 1, False, True)
    attend(1)
    both(1, 0, True, True)
    both(1, 1, True, True)

    def last(q):
        rows = pl.ds(q * 128, 128)
        piece = PIECE[q // 2]
        for at in range(q * 128, q * 128 + 128, piece):
            ps, ms = rbp.at[0, pl.ds(at, piece)], rbm.at[0, pl.ds(at, piece)]
            rcopy(ps, ps, ssem.at[15], rsp.at[0, at // 64], y=up).wait_recv()
            rcopy(ms, ms, ssem.at[16], rsm.at[0, at // 64], y=down).wait_recv()
        v = pb[0, rows, :] + rbp[0, rows, :].astype(f32) + rbm[0, rows, :].astype(f32)
        fin[rows, :] = v.astype(bf16)
        for p in (2 * q, 2 * q + 1):
            for dxs in range(NX):
                at = pl.ds((p * NX + dxs) * CAP, CAP)
                if p == 0 and dxs == 0:
                    res[pl.ds(mine, CAP), :] = fin[0:CAP, :]
                    continue
                rcopy(
                    fin.at[at],
                    res.at[pl.ds(mine, CAP)],
                    ssem.at[18],
                    msem.at[8],
                    z=lax.rem(z + NEAR[p], NZ),
                    x=lax.rem(x + dxs, NX),
                ).start()

    last(1)
    last(0)

    pr0 = pr.at[pl.ds(0, 3 * ROWS_A)]
    rcopy(pr0, pr0, ssem.at[10], msem.at[5], x=x).wait_recv()
    parts = [po[0:ROWS_A, :]] + [pr[k * ROWS_A : (k + 1) * ROWS_A, :] for k in range(1, NX)]
    tops = [p[:, 0:1] for p in parts]
    top = jnp.maximum(jnp.maximum(tops[0], tops[1]), jnp.maximum(tops[2], tops[3]))
    att = sum(p * jnp.exp(t - top) for p, t in zip(parts, tops))
    att = jnp.where(iota((ROWS_A, 128), 1) < HD, 0.0, att)
    mean = jnp.sum(att * att, axis=-1, keepdims=True) * (1.0 / HD)
    head = att * lax.rsqrt(mean + HEAD_FLOOR)
    packed = jnp.where(
        iota((HALF, 128), 1) < HD, pltpu.roll(head[:HALF], HD, 1), head[HALF:]
    )
    hbm[pl.ds(y, 1)] = packed.astype(bf16)[None]
    for dy in (4, 3, 5, 2, 6, 1, 7):
        rcopy(
            hbm.at[y],
            hbm.at[y],
            ssem.at[17],
            msem.at[7 if dy in (3, 4, 5) else 3],
            y=lax.rem(y + dy, NY),
        ).start()

    last(3)
    last(2)

    weights = first * rw[0:1, :] + second * rw[1:2, :]
    spread = exact(pick, weights)
    rest = jnp.where(dispatch[...] > 0.5, spread, 0.0).T
    for k in range(3):
        term = rest.astype(bf16)
        comb[k] = term
        rest = rest - term.astype(f32)
    bw[...] = jnp.zeros_like(bw)
    for h in range(16):
        bw[h * 128 : h * 128 + HD, 0:128] = ow[h * HD : (h + 1) * HD, :]
        bw[h * 128 + HD : h * 128 + 128, 128:256] = ow[h * HD : (h + 1) * HD, :]

    h0 = hbm.at[pl.ds(0, NY - 1)]
    hc = rcopy(hbm, hbo, ssem.at[19], msem.at[9], c=other)
    for sem, offsets in ((3, (0, 1, 7, 2, 6)), (7, (3, 5, 4))):
        some = hbm.at[pl.ds(0, 4 if sem == 3 else 3)]
        rcopy(some, some, ssem.at[17], msem.at[sem], y=up).wait_recv()
        for dy in offsets:
            at = lax.rem(y + dy, NY)
            rcopy(hbm.at[at], hbo.at[at], ssem.at[19], msem.at[9], c=other).start()
    acc = jnp.zeros((HALF, 256), f32)
    for k in range(NY):
        acc = acc + jnp.dot(
            hbm[k], bw[pl.ds(pl.multiple_of((2 * k + c) * 128, 128), 128), :],
            preferred_element_type=f32,
        )

    r0 = res.at[pl.ds(0, SLOTS - CAP)]

    def experts_out():
        rcopy(r0, r0, ssem.at[18], msem.at[8], z=z).wait_recv()
        eo[...] = sum(
            jnp.dot(comb[k], res[...], preferred_element_type=f32) for k in range(3)
        ).astype(bf16)

    def mixer_out():
        hc.wait_recv()
        whole = acc
        for k in range(NY):
            whole = whole + jnp.dot(
                hbo[k], bw[pl.ds(pl.multiple_of((2 * k + other) * 128, 128), 128), :],
                preferred_element_type=f32,
            )
        mo[0:HALF, :] = whole[:, 0:128].astype(bf16)
        mo[HALF:ROWS_A, :] = whole[:, 128:256].astype(bf16)

    @pl.when(c == 0)
    def _():
        mixer_out()
        experts_out()

    @pl.when(c == 1)
    def _():
        experts_out()
        mixer_out()

    def sent(ref, sem):
        rcopy(ref, ref, ssem.at[sem], msem.at[0], c=other).wait_send()

    sent(dw, 0)
    sent(outrows.at[pl.ds(0, SLOTS - CAP)], 1)
    sent(gx0, 2)
    sent(q0, 3)
    sent(kv0, 4)
    sent(gz0, 5)
    for s in (6, 7, 8, 9):
        sent(xm.at[0], s)
    sent(pr0, 10)
    for s in (11, 12, 13):
        sent(xm.at[0], s)
    sent(hid, 14)
    for s in (15, 16):
        sent(sbp.at[pl.ds(0, 14 * 128)], s)
    sent(h0, 17)
    sent(r0, 18)
    sent(hbm, 19)


def on_device(mt, mg, qw, kw, vw, fw, fb, ow, et, eg, rt, rw, gw, uw, dw):
    vmem = pl.BlockSpec(memory_space=pltpu.VMEM)
    hbm = pl.BlockSpec(memory_space=pl.ANY)
    dma = pltpu.SemaphoreType.DMA
    return pl.pallas_call(
        kernel,
        name="mixer_and_experts",
        out_shape=(
            pltpu.VMEM((ROWS_A, 128), bf16),
            pltpu.VMEM((ROWS_B, 128), bf16),
        ),
        in_specs=[hbm] * 15,
        out_specs=(vmem, vmem),
        scratch_shapes=[
            pltpu.VMEM((ROWS_A, D), bf16),
            pltpu.VMEM((1, D), f32),
            pltpu.VMEM((1, D), bf16),
            pltpu.VMEM((1, 1), f32),
            pltpu.VMEM((16 * HD, 128), bf16),
            pltpu.VMEM((ROWS_B, D), bf16),
            pltpu.VMEM((1, D), f32),
            pltpu.VMEM((2, ROWS_B), jnp.int32),
            pltpu.VMEM((2, ROWS_B), f32),
            pltpu.VMEM((FF, D), bf16),
            pltpu.VMEM((FF, D), bf16),
            pltpu.VMEM((FF, D), bf16),
            pltpu.VMEM((FF, D), bf16),
            pltpu.VMEM((4 * HD, D), bf16),
            pltpu.VMEM((ROWS_A, D), bf16),
            pltpu.VMEM((ROWS_B, QUART), bf16),
            pltpu.VMEM((SLOTS, QUART), bf16),
            pltpu.VMEM((SLOTS, ROWS_B), bf16),
            pltpu.VMEM((3, ROWS_B, SLOTS), bf16),
            pltpu.VMEM((4, SLOTS, QUART), bf16),
            pltpu.VMEM((4, SLOTS, QUART), bf16),
            pltpu.VMEM((SLOTS, FF), f32),
            pltpu.VMEM((SLOTS, FF), f32),
            pltpu.VMEM((SLOTS, FF), bf16),
            pltpu.VMEM((SLOTS, FF), bf16),
            pltpu.VMEM((NY, SLOTS, 128), f32),
            pltpu.VMEM((5 * SLOTS, 128), bf16),
            pltpu.VMEM((5 * SLOTS, 128), bf16),
            pltpu.VMEM((4, SLOTS, 128), bf16),
            pltpu.VMEM((4, SLOTS, 128), bf16),
            pltpu.VMEM((SLOTS, 128), bf16),
            pltpu.VMEM((SLOTS, 128), bf16),
            pltpu.VMEM((NX * ROWS_A, 128), bf16),
            pltpu.VMEM((NZ * ROWS_A, 128), bf16),
            pltpu.VMEM((8, 256), f32),
            pltpu.VMEM((NX, 8, 256), f32),
            pltpu.VMEM((8, 256), f32),
            pltpu.VMEM((NZ, 8, 256), f32),
            pltpu.VMEM((8, NZ * ROWS_A), f32),
            pltpu.VMEM((NX * ROWS_A, NZ * ROWS_A), f32),
            pltpu.VMEM((NX * ROWS_A, NZ * ROWS_A), bf16),
            pltpu.VMEM((NX * ROWS_A, 128), f32),
            pltpu.VMEM((NX * ROWS_A, 128), f32),
            pltpu.VMEM((NY, ROWS_A // 2, 128), bf16),
            pltpu.VMEM((NY, ROWS_A // 2, 128), bf16),
            pltpu.VMEM((D, 256), bf16),
            dma((15,)),
            dma((20,)),
            dma((4,)),
            dma((4, 4)),
            dma((4, 2)),
            dma((4, 8)),
            dma((4, 8)),
            dma((2,)),
            dma((11,)),
        ],
        compiler_params=pltpu.CompilerParams(collective_id=0, has_side_effects=True),
        cost_estimate=pl.CostEstimate(
            flops=3_000_000_000, bytes_accessed=6_000_000, transcendentals=1_200_000
        ),
    )(
        mt, mg.reshape(1, D), qw, kw, vw, fw.T, fb, ow, et, eg.reshape(1, D), rt.T, rw.T,
        gw, uw, dw,
    )


def solution(mesh):
    split = Mesh(mesh.devices.reshape(NZ, NX, NY, NC), ("z", "x", "y", "c"))
    return jax.shard_map(
        on_device,
        mesh=split,
        in_specs=(
            P(EP, None),
            P(),
            P(TP, None),
            P(TP, None),
            P(TP, None),
            P(None, TP),
            P(EP, TP),
            P(None, TP),
            P(EP, None),
            P(),
            P(EP, None),
            P(EP, None),
            P(EP, TP, None),
            P(EP, TP, None),
            P(EP, TP, None),
        ),
        out_specs=(P(EP, TP), P(EP, TP)),
        check_vma=False,
    )
```
